256 devices in a mesh: sp: 16 (over y, x), tp: 16 (over z, core).
Axes of the slice: x: 4, y: 4, z: 8, core: 2. Of those that a mesh axis runs over, the one named last changes fastest.
Arguments:
- cotangent: bfloat16 [4096, 2048], P('sp', 'tp'), may hold values from -6 to 6
- block_input: bfloat16 [4096, 2048], P('sp', 'tp'), may hold values from -6 to 6
- routes: int32 [4096, 2], P('sp'), may hold values from 0 to 15, all different within a row; in each aligned block of 256 rows (0 to 255, 256 to 511, ...) at most 40 rows name the same one
- route_weights: float32 [4096, 2], P('sp'), may hold values from 0.1 to 0.9
- gate_weight: bfloat16 [16, 2048, 7168], P('sp', None, 'tp'), may hold values from -0.125 to 0.125
- up_weight: bfloat16 [16, 2048, 7168], P('sp', None, 'tp'), may hold values from -0.125 to 0.125
- down_weight: bfloat16 [16, 7168, 2048], P('sp', 'tp'), may hold values from -0.0625 to 0.0625
- out_weight: bfloat16 [1024, 2048], P('tp'), may hold values from -0.1875 to 0.1875
- conv_out: bfloat16 [1024, 4096], P('tp', 'sp'), may hold values from -6 to 6
- gate_pre: bfloat16 [1024, 4096], P('tp', 'sp'), may hold values from -6 to 6
- prior_states: bfloat16 [1024, 4096], P('tp', 'sp'), may hold values from -6 to 6
- recur_weight: bfloat16 [16, 64, 64], replicated, may hold values from -0.75 to 0.75
- input_gate_matrix: bfloat16 [16, 64, 64], replicated, may hold values from -0.75 to 0.75
- decay_param: float32 [1024], replicated, may hold values from 4 to 16
- decay_jump: float32 [1024, 4096], P('tp', 'sp'), may hold values from -1 to 0, as said below
Outputs:
- gate_weight_grad: bfloat16 [16, 2048, 7168], P('sp', None, 'tp')
- up_weight_grad: bfloat16 [16, 2048, 7168], P('sp', None, 'tp')
- down_weight_grad: bfloat16 [16, 7168, 2048], P('sp', 'tp')
- out_weight_grad: float32 [1024, 2048], P('tp', 'sp')
- conv_grad: bfloat16 [1024, 4096], P('tp', 'sp')
- valve_logit_derivative: bfloat16 [1024, 4096], P('tp', 'sp')
The draws below stay inside these ranges and needn't reach their ends.
Inputs may be any that keep to these rules, and one draw needn't show every extreme that they name: In each aligned block of 256 rows (the rows of one index of sp) no expert is named by more than 40 routes, a bound that some block reaches; a row names 2 different experts. `decay_jump`: every entry is at most -1 / 81920.
All inputs are finite; a program needn't handle non-finite values.
Results may differ from the reference program's by a relative error of at most 0.018.
Values may be sent and summed in bfloat16 or wider, within the bound.
A program may use at most 128 MiB of HBM per device.

```python
import math
import jax
import jax.numpy as jnp
import numpy as np
from jax import lax

D = 2048
HEAD_DIM = 64
HEADS = 16
FF = 7168
TOP_K = 2
TOK_DEV = 256
WIDTH = 1024
EXPERTS = 16
TOKENS = 4096
CAP = 40
N_SP = 16
N_TP = 16


def draw_decay_param(key, part):
    keys = jax.random.split(jax.random.fold_in(key, 11), 3)
    share = 0.5
    fast = jax.random.uniform(keys[0], (WIDTH,), jnp.float32) < share
    fast_rate = jnp.exp(jax.random.uniform(keys[1], (WIDTH,), jnp.float32, jnp.log(1.0 / 400.0), jnp.log(1.0 / 100.0)))
    slow_rate = jnp.exp(jax.random.uniform(keys[2], (WIDTH,), jnp.float32, jnp.log(0.1), jnp.log(0.8))) / (8.0 * TOKENS)
    rate = jnp.where(fast, fast_rate, slow_rate)
    return (-jnp.log(jnp.expm1(rate))).astype(jnp.float32)


def draw_decay_jump(key, part):
    keys = jax.random.split(jax.random.fold_in(key, 23), 3)
    blocks = TOKENS // TOK_DEV
    block_rate = jnp.exp(jax.random.uniform(keys[0], (WIDTH, blocks), jnp.float32, jnp.log(0.05), jnp.log(0.4))) / TOKENS
    settled_regime = jnp.repeat(block_rate, TOK_DEV, axis=1)
    deposit_items = jax.random.randint(keys[1], (2,), 0, TOKENS)
    objective_numbers = jnp.log(jax.random.uniform(keys[2], (WIDTH, 2), jnp.float32, 0.6, 0.8))
    sequence_indices = jnp.arange(TOKENS)[None, :]
    clustered_bundles = jnp.where(sequence_indices == deposit_items[0], objective_numbers[:, 0:1], 0.0) + jnp.where(sequence_indices == deposit_items[1], objective_numbers[:, 1:2], 0.0)
    return (clustered_bundles - settled_regime).astype(jnp.float32)


def spiked(array, stream_key, source, target, blocks, factor):
    def block_of(axis_at):
        return (jnp.arange(array.shape[axis_at]) // (array.shape[axis_at] // blocks)).reshape((-1,) + (1,) * (array.ndim - 1 - axis_at))

    first = jax.random.permutation(stream_key, blocks)[block_of(target)]
    far = (block_of(target) + blocks // 2) % blocks
    return jnp.where((block_of(source) == first) | (block_of(source) == far), factor * array, array)


def steps_of(own_key, dims, cuts, smallest, top_value):
    def one(dim, blocks):
        steps = jax.random.uniform(jax.random.fold_in(jax.random.fold_in(own_key, 6), dim), (blocks,), jnp.float32, smallest / len(cuts), top_value / len(cuts))
        return jnp.repeat(jnp.exp(steps), dims[dim] // blocks).reshape((-1,) + (1,) * (len(dims) - dim - 1))

    factor_of = one(*cuts[0])
    for cut in cuts[1:]:
        factor_of = factor_of * one(*cut)
    return factor_of


def routed_block(own_key, own, number, rows, amount, top, limit, lean):
    order = jax.random.permutation(own_key, amount)
    packed, usual = portions_of(amount, rows * top, limit, lean, True), portions_of(amount, rows * top, limit, lean, False)
    places = jnp.arange(amount)

    def named(lengths, turn):
        used = int((lengths > 0).sum())
        fixed = max(1, used // 4)
        passed = fixed + (places - fixed + turn * (used - fixed)) % max(1, amount - fixed)
        return jnp.zeros((amount,), jnp.int32).at[order[jnp.where(places < fixed, places, passed)]].set(jnp.asarray(lengths, jnp.int32))

    lengths = jnp.where(number % 4 == 0, named(packed, number // 4), named(usual, number - number // 4 - 1))
    mixed = jax.random.permutation(jax.random.fold_in(own, 3), amount)
    donor, taker = mixed[0:amount // 2 * 2:2], mixed[1:amount // 2 * 2:2]
    room = jnp.minimum(lengths[donor] - 1, limit - lengths[taker]) // 2
    room = jnp.where((donor == order[0]) | (taker == order[0]) | (lengths[taker] == 0), 0, jnp.maximum(room, 0))
    passed = jax.random.randint(jax.random.fold_in(own, 4), (amount // 2,), 0, 1 << 20) % (room + 1)
    lengths = lengths.at[donor].add(-passed).at[taker].add(passed)
    items = jnp.searchsorted(jnp.cumsum(lengths), jnp.arange(rows * top), side="right").astype(jnp.int32)
    listing = items.reshape(top, rows).T
    listing = listing[jax.random.permutation(jax.random.fold_in(own, 1), rows)]
    turn = jax.random.randint(jax.random.fold_in(own, 2), (rows, 1), 0, top)
    return jnp.take_along_axis(listing, (jnp.arange(top)[None, :] + turn) % top, axis=1)


def portions_of(amount, total, reach, lean, full):
    loads = [(1 << 20) // math.isqrt(standing ** lean) + 1 for standing in range(1, amount + 1)]
    largest = reach if full else min(reach, max(-(-total // amount), total * loads[0] // sum(loads)))
    least = 1 if total - largest >= amount - 1 else 0
    given, rest = [largest] + [least] * (amount - 1), total - largest - least * (amount - 1)
    while rest > 0:
        free = [i for i in range(1, amount) if given[i] < largest] or [i for i in range(1, amount) if given[i] < reach]
        whole, budget = sum([loads[i] for i in free]), rest
        for i in free:
            extra = min(reach - given[i], max(1, budget * loads[i] // whole), rest)
            given[i] = given[i] + extra
            rest = rest - extra
    return np.array(given)


def noise(own_key, shape, deviation, reach, cuts=(), kind=jnp.bfloat16):
    array = deviation * jax.random.normal(own_key, shape, jnp.float32)
    if cuts:
        array = array * steps_of(own_key, shape, cuts, -0.22, 0.18)
    return jnp.clip(array, -reach, reach).astype(kind)


def heavy_noise(own_key, extent, scale, limit, cuts, heavy, kind=jnp.bfloat16):
    values = scale * jax.random.normal(own_key, extent, jnp.float32)
    if cuts:
        values = values * steps_of(own_key, extent, cuts, -0.22, 0.18)
    return jnp.clip(spiked(values, jax.random.fold_in(own_key, 3), *heavy), -limit, limit).astype(kind)


def setup_inputs(seed: int = 0) -> dict:
    key_of = jax.random.split(jax.random.key(seed), 16)
    cotangent = heavy_noise(key_of[0], (TOKENS, D), 1.0, 6.0, ((0, 16), (1, 16)), (0, 1, 16, 2.0))
    block_input = noise(key_of[1], (TOKENS, D), 1.0, 6.0, ((0, 16), (1, 16)))
    routes_keys = jax.random.split(jax.random.fold_in(key_of[2], 1), TOKENS // TOK_DEV)
    routes_turns = jax.random.permutation(jax.random.fold_in(key_of[2], 3), TOKENS // TOK_DEV)
    routes = jax.vmap(lambda own, number: routed_block(jax.random.fold_in(key_of[2], 2), own, number, TOK_DEV, EXPERTS, TOP_K, CAP, 2))(routes_keys, routes_turns).reshape((TOKENS, TOP_K))
    route_weights = jnp.clip(0.1 + 0.79999997 * jax.random.uniform(key_of[3], (TOKENS, TOP_K), jnp.float32) ** steps_of(key_of[3], (TOKENS, TOP_K), ((0, 16),), -0.2, 0.2), 0.1, 0.9)
    gate_weight = noise(key_of[4], (EXPERTS, D, FF), D ** -0.5, 0.125, ((0, 16), (2, 16)))
    up_weight = noise(key_of[5], (EXPERTS, D, FF), D ** -0.5, 0.125, ((0, 16), (2, 16)))
    down_weight = noise(key_of[6], (EXPERTS, FF, D), FF ** -0.5, 0.0625, ((0, 16), (1, 16)))
    out_weight = noise(key_of[7], (WIDTH, D), WIDTH ** -0.5, 0.1875, ((0, 16),))
    conv_out = noise(key_of[8], (WIDTH, TOKENS), 1.0, 6.0, ((0, 16), (1, 16)))
    gate_pre = noise(key_of[9], (WIDTH, TOKENS), 1.0, 6.0, ((0, 16), (1, 16)))
    prior_states = noise(key_of[10], (WIDTH, TOKENS), 1.0, 6.0, ((0, 16), (1, 16)))
    recur_weight = noise(key_of[11], (HEADS, HEAD_DIM, HEAD_DIM), HEAD_DIM ** -0.5, 0.75)
    input_gate_matrix = noise(key_of[12], (HEADS, HEAD_DIM, HEAD_DIM), HEAD_DIM ** -0.5, 0.75)
    decay_param = draw_decay_param(jax.random.fold_in(key_of[15], 71), 0)
    decay_jump = draw_decay_jump(jax.random.fold_in(key_of[15], 71), 0)
    return dict(cotangent=cotangent, block_input=block_input, routes=routes, route_weights=route_weights, gate_weight=gate_weight, up_weight=up_weight, down_weight=down_weight, out_weight=out_weight, conv_out=conv_out, gate_pre=gate_pre, prior_states=prior_states, recur_weight=recur_weight, input_gate_matrix=input_gate_matrix, decay_param=decay_param, decay_jump=decay_jump)


RATE_SCALE = 8.0

def link_pairs(left_pair, right_pair):
    return (left_pair[0] * right_pair[0], right_pair[0] * left_pair[1] + right_pair[1])

def expert_pass(operands, padded_input, padded_cot):
    index_row, weight_row, w_gate, w_up, w_down = operands
    slot_rows = padded_input[index_row]
    slot_cot = (weight_row[:, None] * padded_cot[index_row].astype(jnp.float32)).astype(jnp.bfloat16)
    gate_act = jnp.dot(slot_rows, w_gate, preferred_element_type=jnp.float32)
    up_act = jnp.dot(slot_rows, w_up, preferred_element_type=jnp.float32)
    sigma_gate = jax.nn.sigmoid(gate_act)
    silu_val = gate_act * sigma_gate
    hidden = (silu_val * up_act).astype(jnp.bfloat16)
    down_grad = jnp.dot(hidden.T, slot_cot, preferred_element_type=jnp.float32).astype(jnp.bfloat16)
    d_hidden = jnp.dot(slot_cot, w_down.T, preferred_element_type=jnp.float32)
    d_gate = (d_hidden * up_act * sigma_gate * (1.0 + gate_act * (1.0 - sigma_gate))).astype(jnp.bfloat16)
    d_up = (d_hidden * silu_val).astype(jnp.bfloat16)
    gate_grad = jnp.dot(slot_rows.T, d_gate, preferred_element_type=jnp.float32).astype(jnp.bfloat16)
    up_grad = jnp.dot(slot_rows.T, d_up, preferred_element_type=jnp.float32).astype(jnp.bfloat16)
    blocks = FF // N_TP
    row_count = index_row.shape[0]
    gate_parts = jnp.einsum('rnf,dnf->nrd', d_gate.astype(jnp.float32).reshape(row_count, N_TP, blocks), w_gate.astype(jnp.float32).reshape(D, N_TP, blocks))
    up_parts = jnp.einsum('rnf,dnf->nrd', d_up.astype(jnp.float32).reshape(row_count, N_TP, blocks), w_up.astype(jnp.float32).reshape(D, N_TP, blocks))
    width_part = lax.optimization_barrier((gate_parts + up_parts).astype(jnp.bfloat16))
    row_grad = lax.optimization_barrier(jnp.sum(width_part.astype(jnp.float32), axis=0)).astype(jnp.bfloat16)
    return (gate_grad, up_grad, down_grad, row_grad)

def reference(cotangent, block_input, routes, route_weights, gate_weight, up_weight, down_weight, out_weight, conv_out, gate_pre, prior_states, recur_weight, input_gate_matrix, decay_param, decay_jump):
    route_count = TOK_DEV * TOP_K
    flat_routes = routes.reshape(N_SP, route_count).astype(jnp.int32)
    onehot = (flat_routes[:, :, None] == jnp.arange(EXPERTS, dtype=jnp.int32)[None, None, :]).astype(jnp.int32)
    slot_rank = lax.optimization_barrier(jnp.sum((jnp.cumsum(onehot, axis=1) - onehot) * onehot, axis=2)).astype(jnp.int32)
    source = jnp.arange(N_SP, dtype=jnp.int32)[:, None]
    position = jnp.arange(route_count, dtype=jnp.int32)[None, :]
    token_ids = (source * TOK_DEV + position // TOP_K).astype(jnp.int32)
    slot_ids = ((flat_routes * N_SP + source) * CAP + slot_rank).astype(jnp.int32)
    total = EXPERTS * N_SP * CAP
    table = jnp.full((total,), TOKENS, jnp.int32).at[slot_ids.reshape(-1)].set(token_ids.reshape(-1))
    weight_table = jnp.zeros((total,), jnp.float32).at[slot_ids.reshape(-1)].set(route_weights.reshape(N_SP, route_count).reshape(-1))
    padded_input = jnp.concatenate([block_input, jnp.zeros((1, D), jnp.bfloat16)], axis=0)
    padded_cot = jnp.concatenate([cotangent, jnp.zeros((1, D), jnp.bfloat16)], axis=0)
    gate_weight_grad, up_weight_grad, down_weight_grad, row_grads = lax.map(partial_expert(padded_input, padded_cot), (table.reshape(EXPERTS, N_SP * CAP), weight_table.reshape(EXPERTS, N_SP * CAP), gate_weight, up_weight, down_weight))
    moe_grad = jnp.zeros((TOKENS + 1, D), jnp.float32).at[table].add(row_grads.reshape(total, D).astype(jnp.float32))[:TOKENS]
    block_grad = (cotangent.astype(jnp.float32) + moe_grad).astype(jnp.bfloat16)
    conv_vals = conv_out.astype(jnp.float32)
    shaped = conv_vals.reshape(HEADS, HEAD_DIM, TOKENS)
    recur_gate = jax.nn.sigmoid(jnp.einsum('hij,hit->hjt', recur_weight.astype(jnp.float32), shaped).reshape(WIDTH, TOKENS))
    input_gate = jax.nn.sigmoid(jnp.einsum('hij,hit->hjt', input_gate_matrix.astype(jnp.float32), shaped).reshape(WIDTH, TOKENS))
    softened = jax.nn.softplus(-decay_param)[:, None]
    log_decay = -RATE_SCALE * recur_gate * softened + decay_jump
    decay_val = jnp.exp(log_decay)
    norm_scale = jnp.sqrt(-jnp.expm1(2.0 * log_decay))
    prior_vals = prior_states.astype(jnp.float32)
    state = decay_val * prior_vals + norm_scale * input_gate * conv_vals
    gate_vals = gate_pre.astype(jnp.float32)
    gelu_val, gelu_pull = jax.vjp(jax.nn.gelu, gate_vals)
    mixed = (gelu_val * state).astype(jnp.bfloat16)
    out_weight_grad = jnp.dot(mixed, block_grad, preferred_element_type=jnp.float32)
    d_mixed = jnp.dot(out_weight, block_grad.T, preferred_element_type=jnp.float32)
    valve_logit_derivative = gelu_pull(d_mixed * state)[0].astype(jnp.bfloat16)
    d_state = d_mixed * gelu_val
    shifted = jnp.concatenate([decay_val[:, 1:], jnp.ones((WIDTH, 1), jnp.float32)], axis=1)
    flipped = lax.associative_scan(link_pairs, (jnp.flip(shifted, 1), jnp.flip(d_state, 1)), axis=1)
    state_grad = jnp.flip(flipped[1], 1)
    grad_log = state_grad * prior_vals * decay_val - state_grad * input_gate * conv_vals * decay_val * decay_val / norm_scale
    grad_recur = (grad_log * -RATE_SCALE * softened * recur_gate * (1.0 - recur_gate)).astype(jnp.bfloat16)
    grad_input = (state_grad * norm_scale * conv_vals * input_gate * (1.0 - input_gate)).astype(jnp.bfloat16)
    back_recur = jnp.einsum('hij,hjt->hit', recur_weight.astype(jnp.float32), grad_recur.astype(jnp.float32).reshape(HEADS, HEAD_DIM, TOKENS)).reshape(WIDTH, TOKENS)
    back_input = jnp.einsum('hij,hjt->hit', input_gate_matrix.astype(jnp.float32), grad_input.astype(jnp.float32).reshape(HEADS, HEAD_DIM, TOKENS)).reshape(WIDTH, TOKENS)
    conv_grad = (state_grad * norm_scale * input_gate + back_recur + back_input).astype(jnp.bfloat16)
    return (gate_weight_grad, up_weight_grad, down_weight_grad, out_weight_grad, conv_grad, valve_logit_derivative)

def partial_expert(padded_input, padded_cot):

    def run_expert(operands):
        return expert_pass(operands, padded_input, padded_cot)
    return run_expert
```

```python
import functools

import jax
import jax.numpy as jnp
from jax import lax
from jax.experimental import pallas as pl
from jax.experimental.pallas import tpu as pltpu
from jax.sharding import Mesh
from jax.sharding import PartitionSpec as P

F32 = jnp.float32
BF16 = jnp.bfloat16
MESH = pl.DeviceIdType.MESH

NY, NX, NZ, NC = 4, 4, 8, 2
NSP = NY * NX
NTP = NZ * NC
HEAD_DIM = 64
CAP = 40
TOK = 256
SLOTS = NSP * CAP
HALF = SLOTS // 2
COL = 128
FFD = 448
RATE_SCALE = 8.0
GELU_A = 0.7978845608028654
GELU_B = 0.044715
REACH = ((NZ // 2, NZ // 2 - 1), (NZ // 2 - 1, NZ // 2))

NT = (((1,), (1,)), ((), ()))
TN = (((0,), (0,)), ((), ()))


def dot(a, b):
    return jnp.dot(a, b, preferred_element_type=F32)


def dot_nt(a, b):
    return lax.dot_general(a, b, NT, preferred_element_type=F32)


def dot_tn(a, b):
    return lax.dot_general(a, b, TN, preferred_element_type=F32)


def minus_expm1(v):
    series = jnp.full_like(v, 1.0)
    for k in range(10, 1, -1):
        series = 1.0 + series * v * (1.0 / k)
    return jnp.where(v > -0.5, -v * series, 1.0 - jnp.exp(v))


def remote(src, dst, send, recv, where):
    return pltpu.make_async_remote_copy(
        src_ref=src, dst_ref=dst, send_sem=send, recv_sem=recv, device_id=where, device_id_type=MESH
    )


def main_kernel(
    routes_ref,
    weights_ref,
    rows_ref,
    cot_ref,
    decay_ref,
    gate_hbm,
    up_hbm,
    down_hbm,
    out_w_hbm,
    conv_hbm,
    pre_hbm,
    prior_hbm,
    jump_hbm,
    recur_hbm,
    input_hbm,
    gathered_hbm,
    acts_hbm,
    out_grad_ref,
    conv_grad_ref,
    valve_ref,
    wg,
    wu,
    wd,
    ow,
    conv_v,
    pre_v,
    prior_v,
    jump_v,
    wr,
    wi,
    sent,
    ag,
    acc_g,
    acc_u,
    acc_d,
    acts,
    own,
    pstage,
    precv,
    ring_out,
    ring_in,
    sums,
    back,
    fg,
    summary,
    summaries,
    ow_out,
    ow_in,
    load_sem,
    a2a_send,
    a2a_recv,
    a2a_self,
    ag_send,
    ag_recv,
    agp_send,
    agp_recv,
    store_sem,
    rp_send,
    rp_recv,
    rr_send,
    rr_recv,
    back_send,
    back_recv,
    back_self,
    fg_send,
    fg_recv,
    fgp_send,
    fgp_recv,
    sum_send,
    sum_recv,
    ow_send,
    ow_recv,
):
    y, x, z, c = (lax.axis_index(n) for n in ("y", "x", "z", "core"))
    s = y * NX + x
    tp = z * NC + c
    mate = {"core": 1 - c}

    def peer(i):
        q = lax.rem(s + i, NSP)
        return q, {"y": q // NX, "x": lax.rem(q, NX)}

    def z_at(o):
        return lax.rem(z + o + 2 * NZ, NZ)

    beside = ({"z": z_at(1)}, {"z": z_at(-1)})

    loads = [
        pltpu.make_async_copy(a, b, load_sem.at[i])
        for i, (a, b) in enumerate(
            (
                (gate_hbm.at[0], wg),
                (up_hbm.at[0], wu),
                (down_hbm.at[0], wd),
                (conv_hbm, conv_v),
                (pre_hbm, pre_v),
                (prior_hbm, prior_v),
                (jump_hbm, jump_v),
                (recur_hbm, wr),
                (input_hbm, wi),
                (out_w_hbm, ow),
            )
        )
    ]
    for load in loads:
        load.start()

    barrier = pltpu.get_barrier_semaphore()
    for i in range(1, NSP):
        pl.semaphore_signal(barrier, inc=1, device_id=peer(i)[1], device_id_type=MESH)
    for where in (*beside, mate):
        pl.semaphore_signal(barrier, inc=1, device_id=where, device_id_type=MESH)

    expert_lane = lax.broadcasted_iota(jnp.int32, (TOK, NSP), 1)
    hot = [(expert_lane == routes_ref[:, k : k + 1]).astype(F32) for k in range(2)]
    tok_sub = lax.broadcasted_iota(jnp.int32, (TOK, TOK), 0)
    tok_lane = lax.broadcasted_iota(jnp.int32, (TOK, TOK), 1)
    earlier = (tok_lane < tok_sub).astype(BF16)
    before = dot(earlier, (hot[0] + hot[1]).astype(BF16))
    targets = [
        jnp.sum(hot[k] * before, axis=1, keepdims=True).astype(jnp.int32)
        + routes_ref[:, k : k + 1] * CAP
        for k in range(2)
    ]
    slot_sub = lax.broadcasted_iota(jnp.int32, (SLOTS, TOK), 0)
    across = [
        jnp.sum(jnp.where(tok_sub == tok_lane, t, 0), axis=0, keepdims=True) for t in targets
    ]
    hits = [(slot_sub == t).astype(F32) for t in across]
    placing = (hits[0] + hits[1]).astype(BF16)
    sent[0] = dot(placing, rows_ref[...]).astype(BF16)
    cot = cot_ref[...].astype(F32)
    sent_cot = dot(hits[0].astype(BF16), (weights_ref[:, 0:1] * cot).astype(BF16)) + dot(
        hits[1].astype(BF16), (weights_ref[:, 1:2] * cot).astype(BF16)
    )
    sent[1] = sent_cot.astype(BF16)

    pl.semaphore_wait(barrier, NSP - 1 + 3)

    def a2a(i, a):
        q, where = peer(i)
        return remote(
            sent.at[a, pl.ds(pl.multiple_of(q * CAP, 8), CAP)],
            ag.at[tp, a, pl.ds(pl.multiple_of(s * CAP, 8), CAP)],
            a2a_send.at[a, i],
            a2a_recv.at[a, i],
            where,
        )

    selfs = []
    for a in range(2):
        for i in range(1, NSP):
            a2a(i, a).start()
        mine = pl.ds(pl.multiple_of(s * CAP, 8), CAP)
        selfs.append(pltpu.make_async_copy(sent.at[a, mine], ag.at[tp, a, mine], a2a_self.at[a]))
        selfs[-1].start()

    def ag_hop(d, k, a):
        o = -k if d == 0 else k
        ref = ag.at[z_at(o) * NC + c, a]
        return remote(ref, ref, ag_send.at[d, k, a], ag_recv.at[d, k, a], beside[d])

    def ag_mate(o, a):
        ref = ag.at[z_at(o) * NC + c, a]
        return remote(ref, ref, agp_send.at[o % NZ, a], agp_recv.at[o % NZ, a], mate)

    loads[0].wait()
    loads[1].wait()
    loads[2].wait()

    for a in range(2):
        for i in range(1, NSP):
            a2a(i, a).wait_recv()
        selfs[a].wait()
        ag_hop(0, 0, a).start()
        ag_hop(1, 0, a).start()
        ag_mate(0, a).start()

    def accumulate(o, first=False):
        for a in range(2):
            ag_mate(o, a).wait_recv()
        zc = z_at(o)
        cols = pl.ds(pl.multiple_of(zc * 2 * COL, 2 * COL), 2 * COL)

        def block(m, _):
            r = pl.ds(pl.multiple_of(m * HALF, HALF), HALF)
            xs = jnp.concatenate([ag[zc * NC, 0, r], ag[zc * NC + 1, 0, r]], axis=1)
            cs = jnp.concatenate([ag[zc * NC, 1, r], ag[zc * NC + 1, 1, r]], axis=1)
            g = dot(xs, wg[cols, :])
            u = dot(xs, wu[cols, :])
            h = dot_nt(cs, wd[:, cols])
            if first:
                acc_g[r, :] = g
                acc_u[r, :] = u
                acc_d[r, :] = h
            else:
                acc_g[r, :] += g
                acc_u[r, :] += u
                acc_d[r, :] += h
            return 0

        lax.fori_loop(0, 2, block, 0)

    for k in range(1, NZ // 2 + 1):
        for a in range(2):
            for d in range(2):
                if k <= REACH[d][a]:
                    ag_hop(d, k - 1, a).wait_recv()
                    if k < REACH[d][a]:
                        ag_hop(d, k, a).start()
                    ag_mate(-k if d == 0 else k, a).start()
        if k == 1:
            accumulate(0, True)
        else:
            accumulate(1 - k)
            accumulate(k - 1)
    accumulate(NZ // 2)

    store = pltpu.make_async_copy(ag, gathered_hbm, store_sem.at[0])
    store.start()

    def act(m, _):
        r = pl.ds(pl.multiple_of(m * 80, 80), 80)
        g = acc_g[r, :]
        u = acc_u[r, :]
        dh = acc_d[r, :]
        sig = jax.nn.sigmoid(g)
        silu = g * sig
        acts[0, r, :] = (silu * u).astype(BF16)
        acts[1, r, :] = (dh * u * sig * (1.0 + g * (1.0 - sig))).astype(BF16)
        acts[2, r, :] = (dh * silu).astype(BF16)
        return 0

    lax.fori_loop(0, SLOTS // 80, act, 0)
    store_acts = pltpu.make_async_copy(acts, acts_hbm, store_sem.at[1])
    store_acts.start()

    def pair_copy(o, a):
        r = pl.ds(a * HALF, HALF)
        return remote(pstage.at[o, r], precv.at[o, r], rp_send.at[o, a], rp_recv.at[o, a], mate)

    def width(o):
        cols = pl.ds(pl.multiple_of(z_at(o) * 2 * COL, 2 * COL), 2 * COL)
        for a in range(2):
            r = pl.ds(a * HALF, HALF)
            part = dot_nt(acts[1, r, :], wg[cols, :]) + dot_nt(acts[2, r, :], wu[cols, :])
            low, high = part[:, :COL], part[:, COL:]
            own[o, r, :] = jnp.where(c == 0, low, high)
            pstage[o, r, :] = jnp.where(c == 0, high, low).astype(BF16)
            pair_copy(o, a).start()

    def paired(o, a):
        pair_copy(o, a).wait_recv()
        r = pl.ds(a * HALF, HALF)
        return own[o, r, :] + precv[o, r, :].astype(F32)

    def rs_hop(d, j, a):
        return remote(
            ring_out.at[d, j, a], ring_in.at[d, j, a], rr_send.at[d, j, a], rr_recv.at[d, j, a], beside[d]
        )

    def rs_step(d, j, a):
        reach = REACH[d][a]
        if j >= reach:
            return
        o = (reach - j) if d == 0 else (j - reach)
        value = paired(o % NZ, a)
        if j > 0:
            rs_hop(d, j - 1, a).wait_recv()
            value = value + ring_in[d, j - 1, a].astype(F32)
        ring_out[d, j, a] = value.astype(BF16)
        rs_hop(d, j, a).start()

    half_way = NZ // 2
    width(half_way)
    width(half_way - 1)
    width(half_way + 1)
    for j in range(half_way):
        rs_step(0, j, 0)
        rs_step(1, j, 1)
        rs_step(0, j, 1)
        rs_step(1, j, 0)
        if j < half_way - 2:
            width(half_way - 2 - j)
            width(half_way + 2 + j)
        if j == half_way - 2:
            width(0)
    for a in range(2):
        r = pl.ds(a * HALF, HALF)
        value = paired(0, a)
        for d in range(2):
            last = REACH[d][a] - 1
            rs_hop(d, last, a).wait_recv()
            value = value + ring_in[d, last, a].astype(F32)
        sums[r, :] = value.astype(BF16)

    def give(i):
        q, where = peer(i)
        return remote(
            sums.at[pl.ds(pl.multiple_of(q * CAP, 8), CAP)],
            back.at[pl.ds(pl.multiple_of(s * CAP, 8), CAP)],
            back_send.at[i],
            back_recv.at[i],
            where,
        )

    for i in range(1, NSP):
        give(i).start()
    mine = pl.ds(pl.multiple_of(s * CAP, 8), CAP)
    keep = pltpu.make_async_copy(sums.at[mine], back.at[mine], back_self.at[0])
    keep.start()

    for load in loads[3:]:
        load.wait()
    sub = lax.broadcasted_iota(jnp.int32, (HEAD_DIM, 2 * HEAD_DIM), 0)
    lane = lax.broadcasted_iota(jnp.int32, (HEAD_DIM, 2 * HEAD_DIM), 1)
    first_lane = lax.rem(tp, 2) * HEAD_DIM
    decay_row = decay_ref[pl.ds(tp // 2, 1), :]
    rate = jnp.sum(jnp.where(lane == sub + first_lane, decay_row, 0.0), axis=1, keepdims=True)
    softened = jnp.maximum(-rate, 0.0) + jnp.log1p(jnp.exp(-jnp.abs(rate)))
    conv_b = conv_v[...]
    conv = conv_b.astype(F32)
    w_recur = wr[tp]
    w_input = wi[tp]
    recur_gate = jax.nn.sigmoid(dot_tn(w_recur, conv_b))
    input_gate = jax.nn.sigmoid(dot_tn(w_input, conv_b))
    log_decay = -RATE_SCALE * recur_gate * softened + jump_v[...]
    decay = jnp.exp(log_decay)
    norm = jnp.sqrt(minus_expm1(2.0 * log_decay))
    prior = prior_v[...].astype(F32)
    state = decay * prior + norm * input_gate * conv
    pre = pre_v[...].astype(F32)
    squared = pre * pre
    t = jnp.tanh(GELU_A * (pre + GELU_B * pre * squared))
    gelu = pre * (0.5 * (1.0 + t))
    d_gelu = 0.5 * (1.0 + t) + 0.5 * pre * (1.0 - t * t) * GELU_A * (1.0 + 3.0 * GELU_B * squared)
    mixed = (gelu * state).astype(BF16)
    time = lax.broadcasted_iota(jnp.int32, (HEAD_DIM, TOK), 1)
    scan_a = [jnp.where(time == TOK - 1, 1.0, pltpu.roll(decay, TOK - 1, 1))]
    reach = 1
    while reach < TOK:
        moved = pltpu.roll(scan_a[-1], TOK - reach, 1)
        scan_a.append(scan_a[-1] * jnp.where(time < TOK - reach, moved, 1.0))
        reach *= 2
    slot_lane = lax.broadcasted_iota(jnp.int32, (TOK, SLOTS), 1)
    gathering = (
        (slot_lane == targets[0]).astype(F32) + (slot_lane == targets[1]).astype(F32)
    ).astype(BF16)

    for i in range(1, NSP):
        give(i).wait_recv()
    keep.wait()
    fg[tp] = (cot + dot(gathering, back[...])).astype(BF16)

    def fg_hop(d, k, a):
        o = -k if d == 0 else k
        ref = fg.at[z_at(o) * NC + c, pl.ds(a * (TOK // 2), TOK // 2)]
        return remote(ref, ref, fg_send.at[d, k, a], fg_recv.at[d, k, a], beside[d])

    def fg_mate(o, a):
        ref = fg.at[z_at(o) * NC + c, pl.ds(a * (TOK // 2), TOK // 2)]
        return remote(ref, ref, fgp_send.at[o % NZ, a], fgp_recv.at[o % NZ, a], mate)

    for a in range(2):
        fg_hop(0, 0, a).start()
        fg_hop(1, 0, a).start()
    for a in range(2):
        fg_mate(0, a).start()

    def mixed_grad(o):
        for a in range(2):
            fg_mate(o, a).wait_recv()
        zc = z_at(o)
        cols = pl.ds(pl.multiple_of(zc * 2 * COL, 2 * COL), 2 * COL)
        grads = jnp.concatenate([fg[zc * NC], fg[zc * NC + 1]], axis=1)
        return dot_nt(ow[:, cols], grads)

    d_mixed = None
    for k in range(1, NZ // 2 + 1):
        for a in range(2):
            for d in range(2):
                if k <= REACH[d][a]:
                    fg_hop(d, k - 1, a).wait_recv()
                    if k < REACH[d][a]:
                        fg_hop(d, k, a).start()
                    fg_mate(-k if d == 0 else k, a).start()
        if k == 1:
            d_mixed = mixed_grad(0)
        else:
            d_mixed = d_mixed + mixed_grad(1 - k)
            d_mixed = d_mixed + mixed_grad(k - 1)
    d_mixed = d_mixed + mixed_grad(NZ // 2)

    valve_ref[...] = (d_gelu * (d_mixed * state)).astype(BF16)
    local_sum = d_mixed * gelu
    reach = 1
    for a in scan_a[:-1]:
        moved = pltpu.roll(local_sum, TOK - reach, 1)
        local_sum = local_sum + a * jnp.where(time < TOK - reach, moved, 0.0)
        reach *= 2
    decay_prod = scan_a[-1]
    head_decay = decay[:, 0:1]
    both = jnp.where(lane < HEAD_DIM, head_decay * decay_prod[:, 0:1], head_decay * local_sum[:, 0:1])
    spot = (lane == sub) | (lane == sub + HEAD_DIM)
    row = jnp.sum(jnp.where(spot, both, 0.0), axis=0, keepdims=True)
    summary[...] = jnp.broadcast_to(row, summary.shape)

    def tell(i):
        return remote(summary, summaries.at[s], sum_send.at[i], sum_recv.at[i], peer(i)[1])

    for i in range(1, NSP):
        tell(i).start()

    def piece(i):
        return remote(ow_out.at[i], ow_in.at[i], ow_send.at[i], ow_recv.at[i], peer(i)[1])

    for i in range(1, NSP):
        q, _ = peer(i)
        ow_out[i] = dot(mixed, fg[q]).astype(BF16)
        piece(i).start()
    total = dot(mixed, fg[s]).astype(BF16).astype(F32)

    for i in range(1, NSP):
        tell(i).wait_recv()
    carried = jnp.zeros((1, 2 * HEAD_DIM), F32)
    for q in range(NSP - 1, 0, -1):
        got = summaries[q, 0:1, :]
        stepped = got + pltpu.roll(got, HEAD_DIM, 1) * carried
        carried = jnp.where(q > s, stepped, carried)
    carry = jnp.sum(jnp.where(lane == sub + HEAD_DIM, carried, 0.0), axis=1, keepdims=True)
    state_grad = local_sum + decay_prod * carry
    grad_log = state_grad * prior * decay - state_grad * input_gate * conv * decay * decay / norm
    grad_recur = (grad_log * -RATE_SCALE * softened * recur_gate * (1.0 - recur_gate)).astype(BF16)
    grad_input = (state_grad * norm * conv * input_gate * (1.0 - input_gate)).astype(BF16)
    conv_grad_ref[...] = (
        state_grad * norm * input_gate + dot(w_recur, grad_recur) + dot(w_input, grad_input)
    ).astype(BF16)

    for i in range(1, NSP):
        piece(i).wait_recv()
        total = total + ow_in[i].astype(F32)
    out_grad_ref[...] = total

    for i in range(1, NSP):
        for a in range(2):
            a2a(i, a).wait_send()
        give(i).wait_send()
        tell(i).wait_send()
        piece(i).wait_send()
    for a in range(2):
        for d in range(2):
            for k in range(REACH[d][a]):
                ag_hop(d, k, a).wait_send()
                fg_hop(d, k, a).wait_send()
                rs_hop(d, k, a).wait_send()
        for o in range(NZ):
            ag_mate(o, a).wait_send()
            fg_mate(o, a).wait_send()
            pair_copy(o, a).wait_send()
    store.wait()
    store_acts.wait()


def grads_kernel(chunk, acts, gate_ref, up_ref, down_ref):
    xs = jnp.concatenate([chunk[0, 0], chunk[1, 0]], axis=1)
    cs = jnp.concatenate([chunk[0, 1], chunk[1, 1]], axis=1)
    gate_ref[0] = dot_tn(xs, acts[1]).astype(BF16)
    up_ref[0] = dot_tn(xs, acts[2]).astype(BF16)
    down_ref[0] = dot_tn(acts[0], cs).astype(BF16)


def weight_grads(gathered, acts):
    width = NTP * COL
    return pl.pallas_call(
        grads_kernel,
        grid=(NZ,),
        in_specs=[
            pl.BlockSpec((NC, 2, SLOTS, COL), lambda j: (j, 0, 0, 0)),
            pl.BlockSpec((3, SLOTS, FFD), lambda j: (0, 0, 0)),
        ],
        out_specs=[
            pl.BlockSpec((1, NC * COL, FFD), lambda j: (0, j, 0)),
            pl.BlockSpec((1, NC * COL, FFD), lambda j: (0, j, 0)),
            pl.BlockSpec((1, FFD, NC * COL), lambda j: (0, 0, j)),
        ],
        out_shape=[
            jax.ShapeDtypeStruct((1, width, FFD), BF16),
            jax.ShapeDtypeStruct((1, width, FFD), BF16),
            jax.ShapeDtypeStruct((1, FFD, width), BF16),
        ],
        name="weight_grads",
    )(gathered, acts)


def local(
    cotangent,
    block_input,
    routes,
    route_weights,
    gate_weight,
    up_weight,
    down_weight,
    out_weight,
    conv_out,
    gate_pre,
    prior_states,
    recur_weight,
    input_gate_matrix,
    decay_param,
    decay_jump,
):
    vmem = pl.BlockSpec(memory_space=pltpu.VMEM)
    hbm = pl.BlockSpec(memory_space=pltpu.HBM)
    dma = pltpu.SemaphoreType.DMA
    hops = NZ // 2
    gathered, acts, out_grad, conv_grad, valve = pl.pallas_call(
        main_kernel,
        in_specs=[vmem] * 5 + [hbm] * 10,
        out_specs=[hbm, hbm, vmem, vmem, vmem],
        out_shape=[
            jax.ShapeDtypeStruct((NTP, 2, SLOTS, COL), BF16),
            jax.ShapeDtypeStruct((3, SLOTS, FFD), BF16),
            jax.ShapeDtypeStruct((HEAD_DIM, COL), F32),
            jax.ShapeDtypeStruct((HEAD_DIM, TOK), BF16),
            jax.ShapeDtypeStruct((HEAD_DIM, TOK), BF16),
        ],
        scratch_shapes=[
            pltpu.VMEM((NTP * COL, FFD), BF16),
            pltpu.VMEM((NTP * COL, FFD), BF16),
            pltpu.VMEM((FFD, NTP * COL), BF16),
            pltpu.VMEM((HEAD_DIM, NTP * COL), BF16),
            pltpu.VMEM((HEAD_DIM, TOK), BF16),
            pltpu.VMEM((HEAD_DIM, TOK), BF16),
            pltpu.VMEM((HEAD_DIM, TOK), BF16),
            pltpu.VMEM((HEAD_DIM, TOK), F32),
            pltpu.VMEM((NTP, HEAD_DIM, HEAD_DIM), BF16),
            pltpu.VMEM((NTP, HEAD_DIM, HEAD_DIM), BF16),
            pltpu.VMEM((2, SLOTS, COL), BF16),
            pltpu.VMEM((NTP, 2, SLOTS, COL), BF16),
            pltpu.VMEM((SLOTS, FFD), F32),
            pltpu.VMEM((SLOTS, FFD), F32),
            pltpu.VMEM((SLOTS, FFD), F32),
            pltpu.VMEM((3, SLOTS, FFD), BF16),
            pltpu.VMEM((NZ, SLOTS, COL), F32),
            pltpu.VMEM((NZ, SLOTS, COL), BF16),
            pltpu.VMEM((NZ, SLOTS, COL), BF16),
            pltpu.VMEM((2, hops, 2, HALF, COL), BF16),
            pltpu.VMEM((2, hops, 2, HALF, COL), BF16),
            pltpu.VMEM((SLOTS, COL), BF16),
            pltpu.VMEM((SLOTS, COL), BF16),
            pltpu.VMEM((NTP, TOK, COL), BF16),
            pltpu.VMEM((8, 2 * HEAD_DIM), F32),
            pltpu.VMEM((NSP, 8, 2 * HEAD_DIM), F32),
            pltpu.VMEM((NSP, HEAD_DIM, COL), BF16),
            pltpu.VMEM((NSP, HEAD_DIM, COL), BF16),
            dma((10,)),
            dma((2, NSP)),
            dma((2, NSP)),
            dma((2,)),
            dma((2, hops, 2)),
            dma((2, hops, 2)),
            dma((NZ, 2)),
            dma((NZ, 2)),
            dma((2,)),
            dma((NZ, 2)),
            dma((NZ, 2)),
            dma((2, hops, 2)),
            dma((2, hops, 2)),
            dma((NSP,)),
            dma((NSP,)),
            dma((1,)),
            dma((2, hops, 2)),
            dma((2, hops, 2)),
            dma((NZ, 2)),
            dma((NZ, 2)),
            dma((NSP,)),
            dma((NSP,)),
            dma((NSP,)),
            dma((NSP,)),
        ],
        compiler_params=pltpu.CompilerParams(
            collective_id=0, has_side_effects=True, vmem_limit_bytes=56 * 1024 * 1024
        ),
        name="exchange",
    )(
        routes,
        route_weights,
        block_input,
        cotangent,
        decay_param.reshape(8, 128),
        gate_weight,
        up_weight,
        down_weight,
        out_weight,
        conv_out,
        gate_pre,
        prior_states,
        decay_jump,
        recur_weight,
        input_gate_matrix,
    )
    gate_grad, up_grad, down_grad = weight_grads(gathered, acts)
    return (gate_grad, up_grad, down_grad, out_grad, conv_grad, valve)


def solution(mesh):
    split = Mesh(mesh.devices.reshape(NY, NX, NZ, NC), ("y", "x", "z", "core"))
    sp, tp = ("y", "x"), ("z", "core")
    return jax.shard_map(
        local,
        mesh=split,
        in_specs=(
            P(sp, tp),
            P(sp, tp),
            P(sp, None),
            P(sp, None),
            P(sp, None, tp),
            P(sp, None, tp),
            P(sp, tp, None),
            P(tp, None),
            P(tp, sp),
            P(tp, sp),
            P(tp, sp),
            P(),
            P(),
            P(),
            P(tp, sp),
        ),
        out_specs=(
            P(sp, None, tp),
            P(sp, None, tp),
            P(sp, tp, None),
            P(tp, sp),
            P(tp, sp),
            P(tp, sp),
        ),
        check_vma=False,
    )
```

```python
import functools

import jax
import jax.numpy as jnp
from jax import lax
from jax.experimental import pallas as pl
from jax.experimental.pallas import tpu as pltpu
from jax.sharding import Mesh
from jax.sharding import PartitionSpec as P

F32 = jnp.float32
BF16 = jnp.bfloat16
MESH = pl.DeviceIdType.MESH
OUT = pltpu.VMEM

NY, NX, NZ, NC = 4, 4, 8, 2
NSP = NY * NX
NTP = NZ * NC
HEAD_DIM = 64
CAP = 40
TOK = 256
SLOTS = NSP * CAP
HALF = SLOTS // 2
COL = 128
FFD = 448
RATE_SCALE = 8.0
GELU_A = 0.7978845608028654
GELU_B = 0.044715
REACH = ((NZ // 2, NZ // 2 - 1), (NZ // 2 - 1, NZ // 2))

NT = (((1,), (1,)), ((), ()))
TN = (((0,), (0,)), ((), ()))


def dot(a, b):
    return jnp.dot(a, b, preferred_element_type=F32)


def dot_nt(a, b):
    return lax.dot_general(a, b, NT, preferred_element_type=F32)


def dot_tn(a, b):
    return lax.dot_general(a, b, TN, preferred_element_type=F32)


def minus_expm1(v):
    series = jnp.full_like(v, 1.0)
    for k in range(10, 1, -1):
        series = 1.0 + series * v * (1.0 / k)
    return jnp.where(v > -0.5, -v * series, 1.0 - jnp.exp(v))


def remote(src, dst, send, recv, where):
    return pltpu.make_async_remote_copy(
        src_ref=src, dst_ref=dst, send_sem=send, recv_sem=recv, device_id=where, device_id_type=MESH
    )


def main_kernel(
    routes_ref,
    weights_ref,
    rows_ref,
    cot_ref,
    decay_ref,
    gate_hbm,
    up_hbm,
    down_hbm,
    out_w_hbm,
    conv_hbm,
    pre_hbm,
    prior_hbm,
    jump_hbm,
    recur_hbm,
    input_hbm,
    gate_out,
    up_out,
    down_out,
    out_grad_ref,
    conv_grad_ref,
    valve_ref,
    wg,
    wu,
    wd,
    ow,
    conv_v,
    pre_v,
    prior_v,
    jump_v,
    wr,
    wi,
    sent,
    ag,
    acc_g,
    acc_u,
    acc_d,
    acts,
    acts_t,
    own,
    pstage,
    precv,
    ring_out,
    ring_in,
    sums,
    back,
    fg,
    summary,
    summaries,
    ow_out,
    ow_in,
    load_sem,
    a2a_send,
    a2a_recv,
    a2a_self,
    ag_send,
    ag_recv,
    agp_send,
    agp_recv,
    rp_send,
    rp_recv,
    rr_send,
    rr_recv,
    back_send,
    back_recv,
    back_self,
    fg_send,
    fg_recv,
    fgp_send,
    fgp_recv,
    sum_send,
    sum_recv,
    ow_send,
    ow_recv,
):
    y, x, z, c = (lax.axis_index(n) for n in ("y", "x", "z", "core"))
    s = y * NX + x
    tp = z * NC + c
    mate = {"core": 1 - c}

    def peer(i):
        q = lax.rem(s + i, NSP)
        return q, {"y": q // NX, "x": lax.rem(q, NX)}

    def z_at(o):
        return lax.rem(z + o + 2 * NZ, NZ)

    beside = ({"z": z_at(1)}, {"z": z_at(-1)})

    loads = [
        pltpu.make_async_copy(a, b, load_sem.at[i])
        for i, (a, b) in enumerate(
            (
                (gate_hbm.at[0], wg),
                (up_hbm.at[0], wu),
                (down_hbm.at[0], wd),
                (conv_hbm, conv_v),
                (pre_hbm, pre_v),
                (prior_hbm, prior_v),
                (jump_hbm, jump_v),
                (recur_hbm, wr),
                (input_hbm, wi),
                (out_w_hbm, ow),
            )
        )
    ]
    for load in loads:
        load.start()

    barrier = pltpu.get_barrier_semaphore()
    for i in range(1, NSP):
        pl.semaphore_signal(barrier, inc=1, device_id=peer(i)[1], device_id_type=MESH)
    for where in (*beside, mate):
        pl.semaphore_signal(barrier, inc=1, device_id=where, device_id_type=MESH)

    expert_sub = lax.broadcasted_iota(jnp.int32, (NSP, TOK), 0)
    hot = [(expert_sub == routes_ref[k : k + 1, :]).astype(F32) for k in range(2)]
    tok_sub = lax.broadcasted_iota(jnp.int32, (TOK, TOK), 0)
    tok_lane = lax.broadcasted_iota(jnp.int32, (TOK, TOK), 1)
    before = dot((hot[0] + hot[1]).astype(BF16), (tok_sub < tok_lane).astype(BF16))
    targets = [
        jnp.sum(hot[k] * before, axis=0, keepdims=True).astype(jnp.int32)
        + routes_ref[k : k + 1, :] * CAP
        for k in range(2)
    ]
    slot_sub = lax.broadcasted_iota(jnp.int32, (SLOTS, TOK), 0)
    hits = [(slot_sub == t).astype(F32) for t in targets]
    placing = (hits[0] + hits[1]).astype(BF16)
    same = tok_sub == tok_lane

    def upright(row):
        return jnp.sum(jnp.where(same, row, jnp.zeros_like(row)), axis=1, keepdims=True)

    sent[0] = dot(placing, rows_ref[...]).astype(BF16)
    cot = cot_ref[...].astype(F32)
    sent_cot = dot(hits[0].astype(BF16), (upright(weights_ref[0:1, :]) * cot).astype(BF16)) + dot(
        hits[1].astype(BF16), (upright(weights_ref[1:2, :]) * cot).astype(BF16)
    )
    sent[1] = sent_cot.astype(BF16)

    pl.semaphore_wait(barrier, NSP - 1 + 3)

    def a2a(i, a):
        q, where = peer(i)
        return remote(
            sent.at[a, pl.ds(pl.multiple_of(q * CAP, 8), CAP)],
            ag.at[tp, a, pl.ds(pl.multiple_of(s * CAP, 8), CAP)],
            a2a_send.at[a, i],
            a2a_recv.at[a, i],
            where,
        )

    selfs = []
    for a in range(2):
        for i in range(1, NSP):
            a2a(i, a).start()
        mine = pl.ds(pl.multiple_of(s * CAP, 8), CAP)
        selfs.append(pltpu.make_async_copy(sent.at[a, mine], ag.at[tp, a, mine], a2a_self.at[a]))
        selfs[-1].start()

    def ag_hop(d, k, a):
        o = -k if d == 0 else k
        ref = ag.at[z_at(o) * NC + c, a]
        return remote(ref, ref, ag_send.at[d, k, a], ag_recv.at[d, k, a], beside[d])

    def ag_mate(o, a):
        ref = ag.at[z_at(o) * NC + c, a]
        return remote(ref, ref, agp_send.at[o % NZ, a], agp_recv.at[o % NZ, a], mate)

    loads[0].wait()
    loads[1].wait()
    loads[2].wait()

    for a in range(2):
        for i in range(1, NSP):
            a2a(i, a).wait_recv()
        selfs[a].wait()
        ag_hop(0, 0, a).start()
        ag_hop(1, 0, a).start()
        ag_mate(0, a).start()

    def accumulate(o, first=False):
        for a in range(2):
            ag_mate(o, a).wait_recv()
        zc = z_at(o)
        cols = pl.ds(pl.multiple_of(zc * 2 * COL, 2 * COL), 2 * COL)

        def block(m, _):
            r = pl.ds(pl.multiple_of(m * HALF, HALF), HALF)
            xs = jnp.concatenate([ag[zc * NC, 0, r], ag[zc * NC + 1, 0, r]], axis=1)
            cs = jnp.concatenate([ag[zc * NC, 1, r], ag[zc * NC + 1, 1, r]], axis=1)
            g = dot_nt(xs, wg[:, cols])
            u = dot_nt(xs, wu[:, cols])
            h = dot_nt(cs, wd[:, cols])
            if first:
                acc_g[r, :] = g
                acc_u[r, :] = u
                acc_d[r, :] = h
            else:
                acc_g[r, :] += g
                acc_u[r, :] += u
                acc_d[r, :] += h
            return 0

        lax.fori_loop(0, 2, block, 0)

    for k in range(1, NZ // 2 + 1):
        for a in range(2):
            for d in range(2):
                if k <= REACH[d][a]:
                    ag_hop(d, k - 1, a).wait_recv()
                    if k < REACH[d][a]:
                        ag_hop(d, k, a).start()
                    ag_mate(-k if d == 0 else k, a).start()
        if k == 1:
            accumulate(0, True)
        else:
            accumulate(1 - k)
            accumulate(k - 1)
    accumulate(NZ // 2)

    def act(m, _):
        r = pl.ds(pl.multiple_of(m * 80, 80), 80)
        g = acc_g[r, :]
        u = acc_u[r, :]
        dh = acc_d[r, :]
        sig = jax.nn.sigmoid(g)
        silu = g * sig
        acts[0, r, :] = (silu * u).astype(BF16)
        acts[1, r, :] = (dh * u * sig * (1.0 + g * (1.0 - sig))).astype(BF16)
        acts[2, r, :] = (dh * silu).astype(BF16)
        return 0

    lax.fori_loop(0, SLOTS // 80, act, 0)
    def pair_copy(o, a):
        r = pl.ds(a * HALF, HALF)
        return remote(pstage.at[o, r], precv.at[o, r], rp_send.at[o, a], rp_recv.at[o, a], mate)

    def width(o):
        cols = pl.ds(pl.multiple_of(z_at(o) * 2 * COL, 2 * COL), 2 * COL)
        for a in range(2):
            r = pl.ds(a * HALF, HALF)
            part = dot(acts[1, r, :], wg[:, cols]) + dot(acts[2, r, :], wu[:, cols])
            low, high = part[:, :COL], part[:, COL:]
            own[o, r, :] = jnp.where(c == 0, low, high)
            pstage[o, r, :] = jnp.where(c == 0, high, low).astype(BF16)
            pair_copy(o, a).start()

    def paired(o, a):
        pair_copy(o, a).wait_recv()
        r = pl.ds(a * HALF, HALF)
        return own[o, r, :] + precv[o, r, :].astype(F32)

    def rs_hop(d, j, a):
        return remote(
            ring_out.at[d, j, a], ring_in.at[d, j, a], rr_send.at[d, j, a], rr_recv.at[d, j, a], beside[d]
        )

    def rs_step(d, j, a):
        reach = REACH[d][a]
        if j >= reach:
            return
        o = (reach - j) if d == 0 else (j - reach)
        value = paired(o % NZ, a)
        if j > 0:
            rs_hop(d, j - 1, a).wait_recv()
            value = value + ring_in[d, j - 1, a].astype(F32)
        ring_out[d, j, a] = value.astype(BF16)
        rs_hop(d, j, a).start()

    def turn(i):
        acts_t[i] = jnp.transpose(acts[i])

    def grads(j):
        cols = slice(j * 2 * COL, (j + 1) * 2 * COL)
        xs = jnp.concatenate([ag[2 * j, 0], ag[2 * j + 1, 0]], axis=1)
        cs = jnp.concatenate([ag[2 * j, 1], ag[2 * j + 1, 1]], axis=1)
        gate_out[0, :, cols] = dot(acts_t[1], xs).astype(BF16)
        up_out[0, :, cols] = dot(acts_t[2], xs).astype(BF16)
        down_out[0, :, cols] = dot(acts_t[0], cs).astype(BF16)

    width(4)
    width(3)
    rs_step(0, 0, 0)
    rs_step(1, 0, 1)
    width(5)
    rs_step(0, 0, 1)
    rs_step(1, 0, 0)
    width(2)
    width(6)
    turn(0)
    for j in range(1, NZ // 2):
        rs_step(0, j, 0)
        rs_step(1, j, 1)
        rs_step(0, j, 1)
        rs_step(1, j, 0)
        if j == 1:
            width(1)
            width(7)
            turn(1)
        if j == 2:
            width(0)
            turn(2)
            grads(0)
        if j == 3:
            grads(1)
            grads(2)
    for a in range(2):
        r = pl.ds(a * HALF, HALF)
        value = paired(0, a)
        for d in range(2):
            last = REACH[d][a] - 1
            rs_hop(d, last, a).wait_recv()
            value = value + ring_in[d, last, a].astype(F32)
        sums[r, :] = value.astype(BF16)

    def give(i):
        q, where = peer(i)
        return remote(
            sums.at[pl.ds(pl.multiple_of(q * CAP, 8), CAP)],
            back.at[pl.ds(pl.multiple_of(s * CAP, 8), CAP)],
            back_send.at[i],
            back_recv.at[i],
            where,
        )

    for i in range(1, NSP):
        give(i).start()
    mine = pl.ds(pl.multiple_of(s * CAP, 8), CAP)
    keep = pltpu.make_async_copy(sums.at[mine], back.at[mine], back_self.at[0])
    keep.start()

    for load in loads[3:]:
        load.wait()
    sub = lax.broadcasted_iota(jnp.int32, (HEAD_DIM, 2 * HEAD_DIM), 0)
    lane = lax.broadcasted_iota(jnp.int32, (HEAD_DIM, 2 * HEAD_DIM), 1)
    first_lane = lax.rem(tp, 2) * HEAD_DIM
    decay_row = decay_ref[pl.ds(tp // 2, 1), :]
    rate = jnp.sum(jnp.where(lane == sub + first_lane, decay_row, 0.0), axis=1, keepdims=True)
    softened = jnp.maximum(-rate, 0.0) + jnp.log1p(jnp.exp(-jnp.abs(rate)))
    conv_b = conv_v[...]
    conv = conv_b.astype(F32)
    w_recur = wr[tp]
    w_input = wi[tp]
    recur_gate = jax.nn.sigmoid(dot_tn(w_recur, conv_b))
    input_gate = jax.nn.sigmoid(dot_tn(w_input, conv_b))
    log_decay = -RATE_SCALE * recur_gate * softened + jump_v[...]
    decay = jnp.exp(log_decay)
    norm = jnp.sqrt(minus_expm1(2.0 * log_decay))
    prior = prior_v[...].astype(F32)
    state = decay * prior + norm * input_gate * conv
    pre = pre_v[...].astype(F32)
    squared = pre * pre
    t = jnp.tanh(GELU_A * (pre + GELU_B * pre * squared))
    gelu = pre * (0.5 * (1.0 + t))
    d_gelu = 0.5 * (1.0 + t) + 0.5 * pre * (1.0 - t * t) * GELU_A * (1.0 + 3.0 * GELU_B * squared)
    mixed = (gelu * state).astype(BF16)
    time = lax.broadcasted_iota(jnp.int32, (HEAD_DIM, TOK), 1)
    scan_a = [jnp.where(time == TOK - 1, 1.0, pltpu.roll(decay, TOK - 1, 1))]
    reach = 1
    while reach < TOK:
        moved = pltpu.roll(scan_a[-1], TOK - reach, 1)
        scan_a.append(scan_a[-1] * jnp.where(time < TOK - reach, moved, 1.0))
        reach *= 2
    slot_lane = lax.broadcasted_iota(jnp.int32, (TOK, SLOTS), 1)
    gathering = (
        (slot_lane == upright(targets[0])).astype(F32)
        + (slot_lane == upright(targets[1])).astype(F32)
    ).astype(BF16)

    grads(3)
    grads(4)
    for i in range(1, NSP):
        give(i).wait_recv()
    keep.wait()
    fg[tp] = (cot + dot(gathering, back[...])).astype(BF16)

    def fg_hop(d, k, a):
        o = -k if d == 0 else k
        ref = fg.at[z_at(o) * NC + c, pl.ds(a * (TOK // 2), TOK // 2)]
        return remote(ref, ref, fg_send.at[d, k, a], fg_recv.at[d, k, a], beside[d])

    def fg_mate(o, a):
        ref = fg.at[z_at(o) * NC + c, pl.ds(a * (TOK // 2), TOK // 2)]
        return remote(ref, ref, fgp_send.at[o % NZ, a], fgp_recv.at[o % NZ, a], mate)

    for a in range(2):
        fg_hop(0, 0, a).start()
        fg_hop(1, 0, a).start()
    for a in range(2):
        fg_mate(0, a).start()

    def mixed_grad(o):
        for a in range(2):
            fg_mate(o, a).wait_recv()
        zc = z_at(o)
        cols = pl.ds(pl.multiple_of(zc * 2 * COL, 2 * COL), 2 * COL)
        grads = jnp.concatenate([fg[zc * NC], fg[zc * NC + 1]], axis=1)
        return dot_nt(ow[:, cols], grads)

    d_mixed = None
    for k in range(1, NZ // 2 + 1):
        for a in range(2):
            for d in range(2):
                if k <= REACH[d][a]:
                    fg_hop(d, k - 1, a).wait_recv()
                    if k < REACH[d][a]:
                        fg_hop(d, k, a).start()
                    fg_mate(-k if d == 0 else k, a).start()
        if k < 4:
            grads(4 + k)
        if k == 1:
            d_mixed = mixed_grad(0)
        else:
            d_mixed = d_mixed + mixed_grad(1 - k)
            d_mixed = d_mixed + mixed_grad(k - 1)
    d_mixed = d_mixed + mixed_grad(NZ // 2)

    valve_ref[...] = (d_gelu * (d_mixed * state)).astype(BF16)
    local_sum = d_mixed * gelu
    reach = 1
    for a in scan_a[:-1]:
        moved = pltpu.roll(local_sum, TOK - reach, 1)
        local_sum = local_sum + a * jnp.where(time < TOK - reach, moved, 0.0)
        reach *= 2
    decay_prod = scan_a[-1]
    head_decay = decay[:, 0:1]
    both = jnp.where(lane < HEAD_DIM, head_decay * decay_prod[:, 0:1], head_decay * local_sum[:, 0:1])
    spot = (lane == sub) | (lane == sub + HEAD_DIM)
    row = jnp.sum(jnp.where(spot, both, 0.0), axis=0, keepdims=True)
    summary[...] = jnp.broadcast_to(row, summary.shape)

    def tell(i):
        return remote(summary, summaries.at[s], sum_send.at[i], sum_recv.at[i], peer(i)[1])

    for i in range(1, NSP):
        tell(i).start()

    def piece(i):
        return remote(ow_out.at[i], ow_in.at[i], ow_send.at[i], ow_recv.at[i], peer(i)[1])

    for i in range(1, NSP):
        q, _ = peer(i)
        ow_out[i] = dot(mixed, fg[q]).astype(BF16)
        piece(i).start()
    total = dot(mixed, fg[s]).astype(BF16).astype(F32)

    for i in range(1, NSP):
        tell(i).wait_recv()
    carried = jnp.zeros((1, 2 * HEAD_DIM), F32)
    for q in range(NSP - 1, 0, -1):
        got = summaries[q, 0:1, :]
        stepped = got + pltpu.roll(got, HEAD_DIM, 1) * carried
        carried = jnp.where(q > s, stepped, carried)
    carry = jnp.sum(jnp.where(lane == sub + HEAD_DIM, carried, 0.0), axis=1, keepdims=True)
    state_grad = local_sum + decay_prod * carry
    grad_log = state_grad * prior * decay - state_grad * input_gate * conv * decay * decay / norm
    grad_recur = (grad_log * -RATE_SCALE * softened * recur_gate * (1.0 - recur_gate)).astype(BF16)
    grad_input = (state_grad * norm * conv * input_gate * (1.0 - input_gate)).astype(BF16)
    conv_grad_ref[...] = (
        state_grad * norm * input_gate + dot(w_recur, grad_recur) + dot(w_input, grad_input)
    ).astype(BF16)

    for i in range(1, NSP):
        piece(i).wait_recv()
        total = total + ow_in[i].astype(F32)
    out_grad_ref[...] = total

    for i in range(1, NSP):
        for a in range(2):
            a2a(i, a).wait_send()
        give(i).wait_send()
        tell(i).wait_send()
        piece(i).wait_send()
    for a in range(2):
        for d in range(2):
            for k in range(REACH[d][a]):
                ag_hop(d, k, a).wait_send()
                fg_hop(d, k, a).wait_send()
                rs_hop(d, k, a).wait_send()
        for o in range(NZ):
            ag_mate(o, a).wait_send()
            fg_mate(o, a).wait_send()
            pair_copy(o, a).wait_send()


def local(
    cotangent,
    block_input,
    routes,
    route_weights,
    gate_weight,
    up_weight,
    down_weight,
    out_weight,
    conv_out,
    gate_pre,
    prior_states,
    recur_weight,
    input_gate_matrix,
    decay_param,
    decay_jump,
):
    vmem = pl.BlockSpec(memory_space=pltpu.VMEM)
    hbm = pl.BlockSpec(memory_space=pltpu.HBM)
    dma = pltpu.SemaphoreType.DMA
    hops = NZ // 2
    gate_grad, up_grad, down_grad, out_grad, conv_grad, valve = pl.pallas_call(
        main_kernel,
        in_specs=[vmem] * 5 + [hbm] * 10,
        out_specs=[vmem] * 6,
        out_shape=[
            OUT((1, FFD, NTP * COL), BF16),
            OUT((1, FFD, NTP * COL), BF16),
            OUT((1, FFD, NTP * COL), BF16),
            OUT((HEAD_DIM, COL), F32),
            OUT((HEAD_DIM, TOK), BF16),
            OUT((HEAD_DIM, TOK), BF16),
        ],
        scratch_shapes=[
            pltpu.VMEM((FFD, NTP * COL), BF16),
            pltpu.VMEM((FFD, NTP * COL), BF16),
            pltpu.VMEM((FFD, NTP * COL), BF16),
            pltpu.VMEM((HEAD_DIM, NTP * COL), BF16),
            pltpu.VMEM((HEAD_DIM, TOK), BF16),
            pltpu.VMEM((HEAD_DIM, TOK), BF16),
            pltpu.VMEM((HEAD_DIM, TOK), BF16),
            pltpu.VMEM((HEAD_DIM, TOK), F32),
            pltpu.VMEM((NTP, HEAD_DIM, HEAD_DIM), BF16),
            pltpu.VMEM((NTP, HEAD_DIM, HEAD_DIM), BF16),
            pltpu.VMEM((2, SLOTS, COL), BF16),
            pltpu.VMEM((NTP, 2, SLOTS, COL), BF16),
            pltpu.VMEM((SLOTS, FFD), F32),
            pltpu.VMEM((SLOTS, FFD), F32),
            pltpu.VMEM((SLOTS, FFD), F32),
            pltpu.VMEM((3, SLOTS, FFD), BF16),
            pltpu.VMEM((3, FFD, SLOTS), BF16),
            pltpu.VMEM((NZ, SLOTS, COL), F32),
            pltpu.VMEM((NZ, SLOTS, COL), BF16),
            pltpu.VMEM((NZ, SLOTS, COL), BF16),
            pltpu.VMEM((2, hops, 2, HALF, COL), BF16),
            pltpu.VMEM((2, hops, 2, HALF, COL), BF16),
            pltpu.VMEM((SLOTS, COL), BF16),
            pltpu.VMEM((SLOTS, COL), BF16),
            pltpu.VMEM((NTP, TOK, COL), BF16),
            pltpu.VMEM((8, 2 * HEAD_DIM), F32),
            pltpu.VMEM((NSP, 8, 2 * HEAD_DIM), F32),
            pltpu.VMEM((NSP, HEAD_DIM, COL), BF16),
            pltpu.VMEM((NSP, HEAD_DIM, COL), BF16),
            dma((10,)),
            dma((2, NSP)),
            dma((2, NSP)),
            dma((2,)),
            dma((2, hops, 2)),
            dma((2, hops, 2)),
            dma((NZ, 2)),
            dma((NZ, 2)),
            dma((NZ, 2)),
            dma((NZ, 2)),
            dma((2, hops, 2)),
            dma((2, hops, 2)),
            dma((NSP,)),
            dma((NSP,)),
            dma((1,)),
            dma((2, hops, 2)),
            dma((2, hops, 2)),
            dma((NZ, 2)),
            dma((NZ, 2)),
            dma((NSP,)),
            dma((NSP,)),
            dma((NSP,)),
            dma((NSP,)),
        ],
        compiler_params=pltpu.CompilerParams(
            collective_id=0, has_side_effects=True, vmem_limit_bytes=56 * 1024 * 1024
        ),
        name="exchange",
    )(
        routes.T,
        route_weights.T,
        block_input,
        cotangent,
        decay_param.reshape(8, 128),
        jnp.swapaxes(gate_weight, 1, 2),
        jnp.swapaxes(up_weight, 1, 2),
        down_weight,
        out_weight,
        conv_out,
        gate_pre,
        prior_states,
        decay_jump,
        recur_weight,
        input_gate_matrix,
    )
    return (
        jnp.swapaxes(gate_grad, 1, 2),
        jnp.swapaxes(up_grad, 1, 2),
        down_grad,
        out_grad,
        conv_grad,
        valve,
    )


def solution(mesh):
    split = Mesh(mesh.devices.reshape(NY, NX, NZ, NC), ("y", "x", "z", "core"))
    sp, tp = ("y", "x"), ("z", "core")
    return jax.shard_map(
        local,
        mesh=split,
        in_specs=(
            P(sp, tp),
            P(sp, tp),
            P(sp, None),
            P(sp, None),
            P(sp, None, tp),
            P(sp, None, tp),
            P(sp, tp, None),
            P(tp, None),
            P(tp, sp),
            P(tp, sp),
            P(tp, sp),
            P(),
            P(),
            P(),
            P(tp, sp),
        ),
        out_specs=(
            P(sp, None, tp),
            P(sp, None, tp),
            P(sp, tp, None),
            P(tp, sp),
            P(tp, sp),
            P(tp, sp),
        ),
        check_vma=False,
    )
```

```python
import functools

import jax
import jax.numpy as jnp
from jax import lax
from jax.experimental import pallas as pl
from jax.experimental.pallas import tpu as pltpu
from jax.sharding import Mesh
from jax.sharding import PartitionSpec as P

F32 = jnp.float32
BF16 = jnp.bfloat16
MESH = pl.DeviceIdType.MESH
OUT = pltpu.VMEM

NY, NX, NZ, NC = 4, 4, 8, 2
NSP = NY * NX
NTP = NZ * NC
HEAD_DIM = 64
CAP = 40
TOK = 256
SLOTS = NSP * CAP
HALF = SLOTS // 2
COL = 128
FFD = 448
RATE_SCALE = 8.0
GELU_A = 0.7978845608028654
GELU_B = 0.044715
REACH = ((NZ // 2, NZ // 2 - 1), (NZ // 2 - 1, NZ // 2))

NT = (((1,), (1,)), ((), ()))
TN = (((0,), (0,)), ((), ()))


def dot(a, b):
    return jnp.dot(a, b, preferred_element_type=F32)


def dot_nt(a, b):
    return lax.dot_general(a, b, NT, preferred_element_type=F32)


def dot_tn(a, b):
    return lax.dot_general(a, b, TN, preferred_element_type=F32)


def minus_expm1(v):
    series = jnp.full_like(v, 1.0)
    for k in range(10, 1, -1):
        series = 1.0 + series * v * (1.0 / k)
    return jnp.where(v > -0.5, -v * series, 1.0 - jnp.exp(v))


def remote(src, dst, send, recv, where):
    return pltpu.make_async_remote_copy(
        src_ref=src, dst_ref=dst, send_sem=send, recv_sem=recv, device_id=where, device_id_type=MESH
    )


def main_kernel(
    routes_ref,
    weights_ref,
    rows_ref,
    cot_ref,
    decay_ref,
    gate_hbm,
    up_hbm,
    down_hbm,
    out_w_hbm,
    conv_hbm,
    pre_hbm,
    prior_hbm,
    jump_hbm,
    recur_hbm,
    input_hbm,
    gate_out,
    up_out,
    down_out,
    out_grad_ref,
    conv_grad_ref,
    valve_ref,
    wg,
    wu,
    wd,
    ow,
    conv_v,
    pre_v,
    prior_v,
    jump_v,
    wr,
    wi,
    sent,
    cots,
    sent_cot,
    ag,
    acc_g,
    acc_u,
    acc_d,
    acts,
    acts_t,
    own,
    pstage,
    precv,
    ring_out,
    ring_in,
    sums,
    back,
    fg,
    summary,
    summaries,
    ow_out,
    ow_in,
    grad_buf,
    load_sem,
    grad_sem,
    a2a_send,
    a2a_recv,
    a2a_self,
    cg_send,
    cg_recv,
    cd_send,
    cd_recv,
    cd_self,
    ag_send,
    ag_recv,
    agp_send,
    agp_recv,
    rp_send,
    rp_recv,
    rr_send,
    rr_recv,
    back_send,
    back_recv,
    back_self,
    fg_send,
    fg_recv,
    fgp_send,
    fgp_recv,
    sum_send,
    sum_recv,
    ow_send,
    ow_recv,
):
    y, x, z, c = (lax.axis_index(n) for n in ("y", "x", "z", "core"))
    s = y * NX + x
    tp = z * NC + c
    mate = {"core": 1 - c}

    def peer(i):
        q = lax.rem(s + i, NSP)
        return q, {"y": q // NX, "x": lax.rem(q, NX)}

    def z_at(o):
        return lax.rem(z + o + 2 * NZ, NZ)

    beside = ({"z": z_at(1)}, {"z": z_at(-1)})

    loads = [
        pltpu.make_async_copy(a, b, load_sem.at[i])
        for i, (a, b) in enumerate(
            (
                (gate_hbm.at[0], wg),
                (up_hbm.at[0], wu),
                (down_hbm.at[0], wd),
                (conv_hbm, conv_v),
                (pre_hbm, pre_v),
                (prior_hbm, prior_v),
                (jump_hbm, jump_v),
                (recur_hbm, wr),
                (input_hbm, wi),
                (out_w_hbm, ow),
            )
        )
    ]
    for load in loads:
        load.start()

    barrier = pltpu.get_barrier_semaphore()
    for i in range(1, NSP):
        pl.semaphore_signal(barrier, inc=1, device_id=peer(i)[1], device_id_type=MESH)
    for where in (*beside, mate):
        pl.semaphore_signal(barrier, inc=1, device_id=where, device_id_type=MESH)

    expert_sub = lax.broadcasted_iota(jnp.int32, (NSP, TOK), 0)
    hot = [(expert_sub == routes_ref[k : k + 1, :]).astype(F32) for k in range(2)]
    tok_sub = lax.broadcasted_iota(jnp.int32, (TOK, TOK), 0)
    tok_lane = lax.broadcasted_iota(jnp.int32, (TOK, TOK), 1)
    before = dot((hot[0] + hot[1]).astype(BF16), (tok_sub < tok_lane).astype(BF16))
    targets = [
        jnp.sum(hot[k] * before, axis=0, keepdims=True).astype(jnp.int32)
        + routes_ref[k : k + 1, :] * CAP
        for k in range(2)
    ]
    slot_sub = lax.broadcasted_iota(jnp.int32, (SLOTS, TOK), 0)
    hits = [(slot_sub == t).astype(F32) for t in targets]
    placing = (hits[0] + hits[1]).astype(BF16)
    same = tok_sub == tok_lane

    def upright(row):
        return jnp.sum(jnp.where(same, row, jnp.zeros_like(row)), axis=1, keepdims=True)

    slot_weight = jnp.sum(
        hits[0] * weights_ref[0:1, :] + hits[1] * weights_ref[1:2, :], axis=1, keepdims=True
    )
    cot = cot_ref[...].astype(F32)

    pl.semaphore_wait(barrier, NSP - 1 + 3)

    def cot_hop(d, k, a):
        o = -k if d == 0 else k
        part = pl.ds(a * (TOK // 2), TOK // 2)
        there = cots.at[z_at(o), part]
        here = cot_ref.at[part] if k == 0 else there
        return remote(here, there, cg_send.at[d, k, a], cg_recv.at[d, k, a], beside[d])

    for a in range(2):
        for d in range(2):
            cot_hop(d, 0, a).start()

    mine = pl.ds(pl.multiple_of(s * CAP, 8), CAP)

    def a2a(i):
        q, where = peer(i)
        return remote(
            sent.at[pl.ds(pl.multiple_of(q * CAP, 8), CAP)],
            ag.at[tp, 0, mine],
            a2a_send.at[i],
            a2a_recv.at[i],
            where,
        )

    first = dot(placing, jnp.concatenate([rows_ref[...], cot_ref[...]], axis=1))
    sent[...] = first[:, :COL].astype(BF16)
    for i in range(1, NSP):
        a2a(i).start()
    rows_self = pltpu.make_async_copy(sent.at[mine], ag.at[tp, 0, mine], a2a_self.at[0])
    rows_self.start()

    def cot_copy(o, i):
        q, where = peer(i)
        zc = z_at(o)
        return remote(
            sent_cot.at[zc, pl.ds(pl.multiple_of(q * CAP, 8), CAP)],
            ag.at[zc * NC + c, 1, mine],
            cd_send.at[o % NZ, i],
            cd_recv.at[o % NZ, i],
            where,
        )

    def cot_self(o):
        zc = z_at(o)
        return pltpu.make_async_copy(
            sent_cot.at[zc, mine], ag.at[zc * NC + c, 1, mine], cd_self.at[o % NZ]
        )

    def send_cot(*offsets):
        if offsets == (0,):
            placed = first[:, COL:]
        else:
            placed = dot(placing, jnp.concatenate([cots[z_at(o)] for o in offsets], axis=1))
        placed = (slot_weight * placed).astype(BF16)
        for n, o in enumerate(offsets):
            sent_cot[z_at(o)] = placed[:, n * COL : (n + 1) * COL]
        for o in offsets:
            cot_self(o).start()

            def one(i, _, o=o):
                cot_copy(o, i).start()
                return 0

            lax.fori_loop(1, NSP, one, 0)

    def got_cot(o):
        def one(i, _):
            cot_copy(o, i).wait_recv()
            return 0

        lax.fori_loop(1, NSP, one, 0)
        cot_self(o).wait()
        ag_mate(o, 1, 0).start()
        ag_mate(o, 1, 1).start()

    def ag_hop(d, k, a):
        o = -k if d == 0 else k
        ref = ag.at[z_at(o) * NC + c, 0, pl.ds(a * HALF, HALF)]
        return remote(ref, ref, ag_send.at[d, k, a], ag_recv.at[d, k, a], beside[d])

    def ag_mate(o, b, a):
        ref = ag.at[z_at(o) * NC + c, b, pl.ds(a * HALF, HALF)]
        return remote(ref, ref, agp_send.at[o % NZ, b, a], agp_recv.at[o % NZ, b, a], mate)

    def cot_step(k):
        for a in range(2):
            for d in range(2):
                if k <= REACH[d][a]:
                    cot_hop(d, k - 1, a).wait_recv()
                    if k < REACH[d][a]:
                        cot_hop(d, k, a).start()

    def rows_step(k, a):
        for d in range(2):
            if k <= REACH[d][a]:
                ag_hop(d, k - 1, a).wait_recv()
                if k < REACH[d][a]:
                    ag_hop(d, k, a).start()
                ag_mate(-k if d == 0 else k, 0, a).start()

    def columns(o):
        return pl.ds(pl.multiple_of(z_at(o) * 2 * COL, 2 * COL), 2 * COL)

    def add_rows(o):
        for a in range(2):
            ag_mate(o, 0, a).wait_recv()
        zc = z_at(o)
        cols = columns(o)

        def block(m, _):
            r = pl.ds(pl.multiple_of(m * HALF, HALF), HALF)
            xs = jnp.concatenate([ag[zc * NC, 0, r], ag[zc * NC + 1, 0, r]], axis=1)
            g = dot_nt(xs, wg[:, cols])
            u = dot_nt(xs, wu[:, cols])
            if o == 0:
                acc_g[r, :] = g
                acc_u[r, :] = u
            else:
                acc_g[r, :] += g
                acc_u[r, :] += u
            return 0

        lax.fori_loop(0, 2, block, 0)

    def add_cot(o):
        for a in range(2):
            ag_mate(o, 1, a).wait_recv()
        zc = z_at(o)
        cols = columns(o)

        def block(m, _):
            r = pl.ds(pl.multiple_of(m * HALF, HALF), HALF)
            cs = jnp.concatenate([ag[zc * NC, 1, r], ag[zc * NC + 1, 1, r]], axis=1)
            h = dot_nt(cs, wd[:, cols])
            if o == 0:
                acc_d[r, :] = h
            else:
                acc_d[r, :] += h
            return 0

        lax.fori_loop(0, 2, block, 0)

    send_cot(0)
    cot_step(1)
    send_cot(-1, 1)
    for i in range(1, NSP):
        a2a(i).wait_recv()
    rows_self.wait()
    for a in range(2):
        ag_hop(0, 0, a).start()
        ag_hop(1, 0, a).start()
    for a in range(2):
        ag_mate(0, 0, a).start()
    cot_step(2)
    send_cot(-2, 2)
    rows_step(1, 0)
    cot_step(3)
    rows_step(1, 1)
    send_cot(-3, 3)
    cot_step(4)
    send_cot(4)
    loads[0].wait()
    loads[1].wait()
    loads[2].wait()
    rows_step(2, 0)
    add_rows(0)
    got_cot(0)
    rows_step(2, 1)
    add_cot(0)
    got_cot(-1)
    got_cot(1)
    add_rows(-1)
    add_cot(-1)
    add_cot(1)
    got_cot(-2)
    got_cot(2)
    rows_step(3, 0)
    add_rows(1)
    add_cot(-2)
    rows_step(3, 1)
    add_cot(2)
    got_cot(-3)
    got_cot(3)
    add_rows(-2)
    add_rows(2)
    rows_step(4, 0)
    got_cot(4)
    add_cot(-3)
    add_cot(3)
    add_rows(-3)
    rows_step(4, 1)
    add_cot(4)
    add_rows(3)
    add_rows(4)

    def act(m, _):
        r = pl.ds(pl.multiple_of(m * 80, 80), 80)
        g = acc_g[r, :]
        u = acc_u[r, :]
        dh = acc_d[r, :]
        sig = jax.nn.sigmoid(g)
        silu = g * sig
        acts[0, r, :] = (silu * u).astype(BF16)
        acts[1, r, :] = (dh * u * sig * (1.0 + g * (1.0 - sig))).astype(BF16)
        acts[2, r, :] = (dh * silu).astype(BF16)
        return 0

    def pair_copy(o, a):
        r = pl.ds(a * HALF, HALF)
        return remote(pstage.at[o, r], precv.at[o, r], rp_send.at[o, a], rp_recv.at[o, a], mate)

    def width(o, a):
        cols = columns(o)
        r = pl.ds(a * HALF, HALF)
        part = dot(acts[1, r, :], wg[:, cols]) + dot(acts[2, r, :], wu[:, cols])
        low, high = part[:, :COL], part[:, COL:]
        own[o, r, :] = jnp.where(c == 0, low, high)
        pstage[o, r, :] = jnp.where(c == 0, high, low).astype(BF16)
        pair_copy(o, a).start()

    def paired(o, a):
        pair_copy(o, a).wait_recv()
        r = pl.ds(a * HALF, HALF)
        return own[o, r, :] + precv[o, r, :].astype(F32)

    def rs_hop(d, j, a):
        return remote(
            ring_out.at[d, j, a], ring_in.at[d, j, a], rr_send.at[d, j, a], rr_recv.at[d, j, a], beside[d]
        )

    def rs_step(d, j, a):
        reach = REACH[d][a]
        if j >= reach:
            return
        o = (reach - j) if d == 0 else (j - reach)
        value = paired(o % NZ, a)
        if j > 0:
            rs_hop(d, j - 1, a).wait_recv()
            value = value + ring_in[d, j - 1, a].astype(F32)
        ring_out[d, j, a] = value.astype(BF16)
        rs_hop(d, j, a).start()

    def turn(i):
        acts_t[i] = jnp.transpose(acts[i])

    def grads(j):
        cols = slice(j * 2 * COL, (j + 1) * 2 * COL)
        xs = jnp.concatenate([ag[2 * j, 0], ag[2 * j + 1, 0]], axis=1)
        cs = jnp.concatenate([ag[2 * j, 1], ag[2 * j + 1, 1]], axis=1)
        grad_buf[0, :, cols] = dot(acts_t[1], xs).astype(BF16)
        grad_buf[1, :, cols] = dot(acts_t[2], xs).astype(BF16)
        grad_buf[2, :, cols] = dot(acts_t[0], cs).astype(BF16)
        for i in range(3):
            grad_copy(j, i).start()

    def grad_copy(j, i):
        cols = pl.ds(j * 2 * COL, 2 * COL)
        out = (gate_out, up_out, down_out)[i]
        return pltpu.make_async_copy(grad_buf.at[i, :, cols], out.at[0, :, cols], grad_sem.at[j, i])

    for a in range(2):
        lax.fori_loop(a * (HALF // 80), (a + 1) * (HALF // 80), act, 0)
        width(4, a)
    rs_step(0, 0, 0)
    width(3, 1)
    rs_step(1, 0, 1)
    width(5, 0)
    rs_step(0, 0, 1)
    width(3, 0)
    rs_step(1, 0, 0)
    width(5, 1)
    width(2, 1)
    width(6, 0)
    for j in range(1, NZ // 2):
        rs_step(0, j, 0)
        rs_step(1, j, 1)
        rs_step(0, j, 1)
        rs_step(1, j, 0)
        if j == 1:
            width(2, 0)
            width(6, 1)
            width(1, 1)
            width(7, 0)
        if j == 2:
            width(1, 0)
            width(7, 1)
            width(0, 0)
            width(0, 1)
        if j == 3:
            for i in range(3):
                turn(i)
    for a in range(2):
        r = pl.ds(a * HALF, HALF)
        value = paired(0, a)
        for d in range(2):
            last = REACH[d][a] - 1
            rs_hop(d, last, a).wait_recv()
            value = value + ring_in[d, last, a].astype(F32)
        sums[r, :] = value.astype(BF16)

    def give(i):
        q, where = peer(i)
        return remote(
            sums.at[pl.ds(pl.multiple_of(q * CAP, 8), CAP)],
            back.at[pl.ds(pl.multiple_of(s * CAP, 8), CAP)],
            back_send.at[i],
            back_recv.at[i],
            where,
        )

    for i in range(1, NSP):
        give(i).start()
    keep = pltpu.make_async_copy(sums.at[mine], back.at[mine], back_self.at[0])
    keep.start()

    for load in loads[3:]:
        load.wait()
    sub = lax.broadcasted_iota(jnp.int32, (HEAD_DIM, 2 * HEAD_DIM), 0)
    lane = lax.broadcasted_iota(jnp.int32, (HEAD_DIM, 2 * HEAD_DIM), 1)
    first_lane = lax.rem(tp, 2) * HEAD_DIM
    decay_row = decay_ref[pl.ds(tp // 2, 1), :]
    rate = jnp.sum(jnp.where(lane == sub + first_lane, decay_row, 0.0), axis=1, keepdims=True)
    softened = jnp.maximum(-rate, 0.0) + jnp.log1p(jnp.exp(-jnp.abs(rate)))
    conv_b = conv_v[...]
    conv = conv_b.astype(F32)
    w_recur = wr[tp]
    w_input = wi[tp]
    recur_gate = jax.nn.sigmoid(dot_tn(w_recur, conv_b))
    input_gate = jax.nn.sigmoid(dot_tn(w_input, conv_b))
    log_decay = -RATE_SCALE * recur_gate * softened + jump_v[...]
    decay = jnp.exp(log_decay)
    norm = jnp.sqrt(minus_expm1(2.0 * log_decay))
    prior = prior_v[...].astype(F32)
    state = decay * prior + norm * input_gate * conv
    pre = pre_v[...].astype(F32)
    squared = pre * pre
    t = jnp.tanh(GELU_A * (pre + GELU_B * pre * squared))
    gelu = pre * (0.5 * (1.0 + t))
    d_gelu = 0.5 * (1.0 + t) + 0.5 * pre * (1.0 - t * t) * GELU_A * (1.0 + 3.0 * GELU_B * squared)
    mixed = (gelu * state).astype(BF16)
    time = lax.broadcasted_iota(jnp.int32, (HEAD_DIM, TOK), 1)
    scan_a = [jnp.where(time == TOK - 1, 1.0, pltpu.roll(decay, TOK - 1, 1))]
    reach = 1
    while reach < TOK:
        moved = pltpu.roll(scan_a[-1], TOK - reach, 1)
        scan_a.append(scan_a[-1] * jnp.where(time < TOK - reach, moved, 1.0))
        reach *= 2
    slot_lane = lax.broadcasted_iota(jnp.int32, (TOK, SLOTS), 1)
    gathering = (
        (slot_lane == upright(targets[0])).astype(F32)
        + (slot_lane == upright(targets[1])).astype(F32)
    ).astype(BF16)

    for j in range(4):
        grads(j)
    for i in range(1, NSP):
        give(i).wait_recv()
    keep.wait()
    fg[tp] = (cot + dot(gathering, back[...])).astype(BF16)

    def fg_hop(d, k, a):
        o = -k if d == 0 else k
        ref = fg.at[z_at(o) * NC + c, pl.ds(a * (TOK // 4), TOK // 4)]
        return remote(ref, ref, fg_send.at[d, k, a], fg_recv.at[d, k, a], beside[d])

    def fg_mate(o, a):
        ref = fg.at[z_at(o) * NC + c, pl.ds(a * (TOK // 4), TOK // 4)]
        return remote(ref, ref, fgp_send.at[o % NZ, a], fgp_recv.at[o % NZ, a], mate)

    for a in range(4):
        fg_hop(0, 0, a).start()
        fg_hop(1, 0, a).start()
    for a in range(4):
        fg_mate(0, a).start()

    def piece(i):
        return remote(ow_out.at[i], ow_in.at[i], ow_send.at[i], ow_recv.at[i], peer(i)[1])

    def pieces(o):
        zc = z_at(o)
        both = jnp.concatenate([fg[zc * NC], fg[zc * NC + 1]], axis=1)
        found = dot(mixed, both).astype(BF16)
        for h in range(NC):
            i = lax.rem(zc * NC + h + NSP - s, NSP)
            ow_out[i] = found[:, h * COL : (h + 1) * COL]

            @pl.when(i != 0)
            def _():
                piece(i).start()

    def mixed_grad(o):
        for a in range(4):
            fg_mate(o, a).wait_recv()
        zc = z_at(o)
        both = jnp.concatenate([fg[zc * NC], fg[zc * NC + 1]], axis=1)
        return dot_nt(ow[:, columns(o)], both)

    d_mixed = None
    for k in range(1, NZ // 2 + 1):
        for a in range(4):
            for d in range(2):
                if k <= REACH[d][a // 2]:
                    fg_hop(d, k - 1, a).wait_recv()
                    if k < REACH[d][a // 2]:
                        fg_hop(d, k, a).start()
                    fg_mate(-k if d == 0 else k, a).start()
        if k < 3:
            grads(3 + k)
        if k == 1:
            d_mixed = mixed_grad(0)
            pieces(0)
        else:
            d_mixed = d_mixed + mixed_grad(1 - k)
            d_mixed = d_mixed + mixed_grad(k - 1)
            if k < 4:
                pieces(1 - k)
                pieces(k - 1)
    d_mixed = d_mixed + mixed_grad(NZ // 2)

    valve_ref[...] = (d_gelu * (d_mixed * state)).astype(BF16)
    local_sum = d_mixed * gelu
    reach = 1
    for a in scan_a[:-1]:
        moved = pltpu.roll(local_sum, TOK - reach, 1)
        local_sum = local_sum + a * jnp.where(time < TOK - reach, moved, 0.0)
        reach *= 2
    decay_prod = scan_a[-1]
    head_decay = decay[:, 0:1]
    both = jnp.where(lane < HEAD_DIM, head_decay * decay_prod[:, 0:1], head_decay * local_sum[:, 0:1])
    spot = (lane == sub) | (lane == sub + HEAD_DIM)
    row = jnp.sum(jnp.where(spot, both, 0.0), axis=0, keepdims=True)
    summary[...] = jnp.broadcast_to(row, summary.shape)

    def tell(i):
        return remote(summary, summaries.at[s], sum_send.at[i], sum_recv.at[i], peer(i)[1])

    for i in range(1, NSP):
        tell(i).start()
    for o in (-3, 3, 4):
        pieces(o)
    grads(6)
    grads(7)

    for i in range(1, NSP):
        tell(i).wait_recv()
    carried = jnp.zeros((1, 2 * HEAD_DIM), F32)
    for q in range(NSP - 1, 0, -1):
        got = summaries[q, 0:1, :]
        stepped = got + pltpu.roll(got, HEAD_DIM, 1) * carried
        carried = jnp.where(q > s, stepped, carried)
    carry = jnp.sum(jnp.where(lane == sub + HEAD_DIM, carried, 0.0), axis=1, keepdims=True)
    state_grad = local_sum + decay_prod * carry
    grad_log = state_grad * prior * decay - state_grad * input_gate * conv * decay * decay / norm
    grad_recur = (grad_log * -RATE_SCALE * softened * recur_gate * (1.0 - recur_gate)).astype(BF16)
    grad_input = (state_grad * norm * conv * input_gate * (1.0 - input_gate)).astype(BF16)
    conv_grad_ref[...] = (
        state_grad * norm * input_gate + dot(w_recur, grad_recur) + dot(w_input, grad_input)
    ).astype(BF16)

    total = ow_out[0].astype(F32)
    for i in range(1, NSP):
        piece(i).wait_recv()
        total = total + ow_in[i].astype(F32)
    out_grad_ref[...] = total

    for j in range(NZ):
        for i in range(3):
            grad_copy(j, i).wait()
    for i in range(1, NSP):
        a2a(i).wait_send()
        give(i).wait_send()
        tell(i).wait_send()
        piece(i).wait_send()
    def left(i, _):
        for o in range(NZ):
            cot_copy(o, i).wait_send()
        return 0

    lax.fori_loop(1, NSP, left, 0)
    for a in range(2):
        for d in range(2):
            for k in range(REACH[d][a]):
                ag_hop(d, k, a).wait_send()
                cot_hop(d, k, a).wait_send()
                fg_hop(d, k, 2 * a).wait_send()
                fg_hop(d, k, 2 * a + 1).wait_send()
                rs_hop(d, k, a).wait_send()
        for o in range(NZ):
            ag_mate(o, 0, a).wait_send()
            ag_mate(o, 1, a).wait_send()
            fg_mate(o, 2 * a).wait_send()
            fg_mate(o, 2 * a + 1).wait_send()
            pair_copy(o, a).wait_send()


def write_kernel(*refs):
    sources, targets, sem = refs[:6], refs[6:12], refs[12]
    copies = [pltpu.make_async_copy(a, b, sem.at[i]) for i, (a, b) in enumerate(zip(sources, targets))]
    for copy in copies:
        copy.start()
    for copy in copies:
        copy.wait()


def written(results):
    return pl.pallas_call(
        write_kernel,
        in_specs=[pl.BlockSpec(memory_space=pl.ANY)] * 6,
        out_specs=[pl.BlockSpec(memory_space=pltpu.HBM)] * 6,
        out_shape=[jax.ShapeDtypeStruct(r.shape, r.dtype) for r in results],
        scratch_shapes=[pltpu.SemaphoreType.DMA((6,))],
        compiler_params=pltpu.CompilerParams(vmem_limit_bytes=1024 * 1024),
        name="write",
    )(*results)


def local(
    cotangent,
    block_input,
    routes,
    route_weights,
    gate_weight,
    up_weight,
    down_weight,
    out_weight,
    conv_out,
    gate_pre,
    prior_states,
    recur_weight,
    input_gate_matrix,
    decay_param,
    decay_jump,
):
    vmem = pl.BlockSpec(memory_space=pltpu.VMEM)
    hbm = pl.BlockSpec(memory_space=pltpu.HBM)
    dma = pltpu.SemaphoreType.DMA
    hops = NZ // 2
    results = pl.pallas_call(
        main_kernel,
        in_specs=[vmem] * 5 + [hbm] * 10,
        out_specs=[pl.BlockSpec(memory_space=pl.ANY)] * 3 + [vmem] * 3,
        out_shape=[
            OUT((1, FFD, NTP * COL), BF16),
            OUT((1, FFD, NTP * COL), BF16),
            OUT((1, FFD, NTP * COL), BF16),
            OUT((HEAD_DIM, COL), F32),
            OUT((HEAD_DIM, TOK), BF16),
            OUT((HEAD_DIM, TOK), BF16),
        ],
        scratch_shapes=[
            pltpu.VMEM((FFD, NTP * COL), BF16),
            pltpu.VMEM((FFD, NTP * COL), BF16),
            pltpu.VMEM((FFD, NTP * COL), BF16),
            pltpu.VMEM((HEAD_DIM, NTP * COL), BF16),
            pltpu.VMEM((HEAD_DIM, TOK), BF16),
            pltpu.VMEM((HEAD_DIM, TOK), BF16),
            pltpu.VMEM((HEAD_DIM, TOK), BF16),
            pltpu.VMEM((HEAD_DIM, TOK), F32),
            pltpu.VMEM((NTP, HEAD_DIM, HEAD_DIM), BF16),
            pltpu.VMEM((NTP, HEAD_DIM, HEAD_DIM), BF16),
            pltpu.VMEM((SLOTS, COL), BF16),
            pltpu.VMEM((NZ, TOK, COL), BF16),
            pltpu.VMEM((NZ, SLOTS, COL), BF16),
            pltpu.VMEM((NTP, 2, SLOTS, COL), BF16),
            pltpu.VMEM((SLOTS, FFD), F32),
            pltpu.VMEM((SLOTS, FFD), F32),
            pltpu.VMEM((SLOTS, FFD), F32),
            pltpu.VMEM((3, SLOTS, FFD), BF16),
            pltpu.VMEM((3, FFD, SLOTS), BF16),
            pltpu.VMEM((NZ, SLOTS, COL), F32),
            pltpu.VMEM((NZ, SLOTS, COL), BF16),
            pltpu.VMEM((NZ, SLOTS, COL), BF16),
            pltpu.VMEM((2, hops, 2, HALF, COL), BF16),
            pltpu.VMEM((2, hops, 2, HALF, COL), BF16),
            pltpu.VMEM((SLOTS, COL), BF16),
            pltpu.VMEM((SLOTS, COL), BF16),
            pltpu.VMEM((NTP, TOK, COL), BF16),
            pltpu.VMEM((8, 2 * HEAD_DIM), F32),
            pltpu.VMEM((NSP, 8, 2 * HEAD_DIM), F32),
            pltpu.VMEM((NSP, HEAD_DIM, COL), BF16),
            pltpu.VMEM((NSP, HEAD_DIM, COL), BF16),
            pltpu.VMEM((3, FFD, NTP * COL), BF16),
            dma((10,)),
            dma((NZ, 3)),
            dma((NSP,)),
            dma((NSP,)),
            dma((1,)),
            dma((2, hops, 2)),
            dma((2, hops, 2)),
            dma((NZ, NSP)),
            dma((NZ, NSP)),
            dma((NZ,)),
            dma((2, hops, 2)),
            dma((2, hops, 2)),
            dma((NZ, 2, 2)),
            dma((NZ, 2, 2)),
            dma((NZ, 2)),
            dma((NZ, 2)),
            dma((2, hops, 2)),
            dma((2, hops, 2)),
            dma((NSP,)),
            dma((NSP,)),
            dma((1,)),
            dma((2, hops, 4)),
            dma((2, hops, 4)),
            dma((NZ, 4)),
            dma((NZ, 4)),
            dma((NSP,)),
            dma((NSP,)),
            dma((NSP,)),
            dma((NSP,)),
        ],
        compiler_params=pltpu.CompilerParams(
            collective_id=0, has_side_effects=True, vmem_limit_bytes=57 * 1024 * 1024
        ),
        name="exchange",
    )(
        routes.T,
        route_weights.T,
        block_input,
        cotangent,
        decay_param.reshape(8, 128),
        jnp.swapaxes(gate_weight, 1, 2),
        jnp.swapaxes(up_weight, 1, 2),
        down_weight,
        out_weight,
        conv_out,
        gate_pre,
        prior_states,
        decay_jump,
        recur_weight,
        input_gate_matrix,
    )
    gate_grad, up_grad, down_grad, out_grad, conv_grad, valve = written(results)
    return (
        jnp.swapaxes(gate_grad, 1, 2),
        jnp.swapaxes(up_grad, 1, 2),
        down_grad,
        out_grad,
        conv_grad,
        valve,
    )


def solution(mesh):
    split = Mesh(mesh.devices.reshape(NY, NX, NZ, NC), ("y", "x", "z", "core"))
    sp, tp = ("y", "x"), ("z", "core")
    return jax.shard_map(
        local,
        mesh=split,
        in_specs=(
            P(sp, tp),
            P(sp, tp),
            P(sp, None),
            P(sp, None),
            P(sp, None, tp),
            P(sp, None, tp),
            P(sp, tp, None),
            P(tp, None),
            P(tp, sp),
            P(tp, sp),
            P(tp, sp),
            P(),
            P(),
            P(),
            P(tp, sp),
        ),
        out_specs=(
            P(sp, None, tp),
            P(sp, None, tp),
            P(sp, tp, None),
            P(tp, sp),
            P(tp, sp),
            P(tp, sp),
        ),
        check_vma=False,
    )
```
